128 devices in a mesh: sp: 32 (over z, y, core), tp: 4 (over x).
Axes of the slice: x: 4, y: 4, z: 4, core: 2. Of those that a mesh axis runs over, the one named last changes fastest.
Arguments:
- resid: bfloat16 [16384, 2048], P(('sp', 'tp')), may hold values from -6 to 6
- query: bfloat16 [16384, 2048], P('sp', 'tp'), may hold values from -6 to 6
- forget_logits: bfloat16 [16384, 2048], P('sp', 'tp'), may hold values from -5 to 5
- forget_margin: float32 [2048], P('tp'), may hold values from 0 to 0.07, as said below
- decay_spike: float32 [16384, 16], P('sp', 'tp'), may hold values from -0.75 to 0
- value_logits: bfloat16 [16384, 2048], P('sp', 'tp'), may hold values from -6 to 6
- output_gate_logits: bfloat16 [16384, 2048], P('sp', 'tp'), may hold values from -6 to 6
- head_norm_scale: float32 [2048], P('tp'), may hold values from 0.1 to 1.9
- output_matrix: bfloat16 [2048, 2048], replicated, may hold values from -0.125 to 0.125
- norm_scale_vector: float32 [2048], replicated, may hold values from 0.1 to 1.9
- routes: int32 [16384, 2], P(('sp', 'tp')), may hold values from 0 to 127, all different within a row; in each aligned block of 128 rows (0 to 127, 128 to 255, ...) at most 4 rows name the same one
- routing_weight: float32 [16384, 2], P(('sp', 'tp')), may hold values from 0.2 to 1
- gate_matrix: bfloat16 [128, 2048, 1024], P(('sp', 'tp')), may hold values from -0.125 to 0.125
- up_matrix: bfloat16 [128, 2048, 1024], P(('sp', 'tp')), may hold values from -0.125 to 0.125
- down_matrix: bfloat16 [128, 1024, 2048], P(('sp', 'tp')), may hold values from -0.1875 to 0.1875
Outputs:
- result: bfloat16 [16384, 2048], P(('sp', 'tp'))
The draws below stay inside these ranges and needn't reach their ends.
Inputs may be any that keep to these rules, and one draw needn't show every extreme that they name: `routes`: within the rows of one device no expert is named by more than 4 rows; some device names some expert exactly 4 times in every draw. `forget_margin`: Positive.
All inputs are finite; a program needn't handle non-finite values.
Results may differ from the reference program's by a relative error of at most 0.012.
Values may be sent and summed in bfloat16 or wider, within the bound.
A program may use at most 128 MiB of HBM per device.

```python
import math
import jax
import jax.numpy as jnp
import numpy as np
from jax import lax

D = 2048
HEAD_TOTAL = 16
DK = 128
DV = 128
FF = 1024
TOP = 2
BLOCK = 64
TOKENS_PER_SHARD = 512
SEQUENCE_TOKENS = 16384
ROWS = 128
EXPERTS = 128
CAP = 4
DEVICES = 128


def slow_choice(key):
    pick_key, slow_key, fast_key = jax.random.split(jax.random.fold_in(key, 11), 3)
    ranking = jax.random.permutation(pick_key, HEAD_TOTAL)
    slow_heads = ranking < HEAD_TOTAL // 2
    return (slow_heads, slow_key, fast_key)


def draw_forget_margin(key, part):
    slow_heads, slow_key, fast_key = slow_choice(key)
    slow_gap = jnp.exp(jax.random.uniform(slow_key, (HEAD_TOTAL, DK), jnp.float32, jnp.log(0.3), jnp.log(1.5))) / SEQUENCE_TOKENS
    fast_gap = jnp.exp(jax.random.uniform(fast_key, (HEAD_TOTAL, DK), jnp.float32, jnp.log(0.02), jnp.log(0.066)))
    return jnp.where(slow_heads[:, None], slow_gap, fast_gap).reshape(HEAD_TOTAL * DK)


def draw_forget_logits(key, part):
    jitter_key, shift_key = jax.random.split(jax.random.fold_in(key, 23))
    block_count = SEQUENCE_TOKENS // TOKENS_PER_SHARD
    shifts = jax.random.uniform(shift_key, (block_count, HEAD_TOTAL), jnp.float32, -1.0, 1.0)
    jitter = jnp.clip(jax.random.normal(jitter_key, (SEQUENCE_TOKENS, HEAD_TOTAL * DK), jnp.float32), -4.0, 4.0)
    block_shift = jnp.repeat(jnp.repeat(shifts, TOKENS_PER_SHARD, axis=0), DK, axis=1)
    return (jitter + block_shift).astype(jnp.bfloat16)


def draw_decay_spike(key, part):
    slow_heads, slow_key, fast_key = slow_choice(key)
    position_seed, spike_size_seed, rate_seed = jax.random.split(jax.random.fold_in(key, 37), 3)
    spike_positions = jax.random.randint(position_seed, (3, HEAD_TOTAL), 0, SEQUENCE_TOKENS)
    spike_magnitudes = jnp.log(jax.random.uniform(spike_size_seed, (3, HEAD_TOTAL), jnp.float32, 0.5, 0.8))
    position_entries = jnp.arange(SEQUENCE_TOKENS, dtype=jnp.int32)[:, None, None] == spike_positions[None, :, :]
    spike_events = jnp.sum(jnp.where(position_entries, spike_magnitudes[None, :, :], 0.0), axis=1)
    block_count = SEQUENCE_TOKENS // TOKENS_PER_SHARD
    additional_rate = -jax.random.uniform(rate_seed, (block_count, HEAD_TOTAL), jnp.float32, 0.005, 0.045)
    additional_rate = jnp.where(slow_heads[None, :], 0.0, additional_rate)
    return spike_events + jnp.repeat(additional_rate, TOKENS_PER_SHARD, axis=0)


def shard_levels(own_key, extent, pieces, low, top_value):
    gain = 1.0
    for axis_at, blocks in pieces:
        draws = jax.random.uniform(jax.random.fold_in(jax.random.fold_in(own_key, 6), axis_at), (blocks,), jnp.float32, low / len(pieces), top_value / len(pieces))
        gain = gain * jnp.repeat(jnp.exp(draws), extent[axis_at] // blocks).reshape((-1,) + (1,) * (len(extent) - 1 - axis_at))
    return gain


def shared_out(stream_key, own, number, rows, amount, top, reach, slope):
    order = jax.random.permutation(stream_key, amount)
    heavy_load, common = load_shares(amount, rows * top, reach, slope, True), load_shares(amount, rows * top, reach, slope, False)
    places = jnp.arange(amount)

    def named(sizes, offset_by):
        used = int((sizes > 0).sum())
        fixed = max(1, used // 4)
        passed = fixed + (places - fixed + offset_by * (used - fixed)) % max(1, amount - fixed)
        return jnp.zeros((amount,), jnp.int32).at[order[jnp.where(places < fixed, places, passed)]].set(jnp.asarray(sizes, jnp.int32))

    sizes = jnp.where(number % 4 == 0, named(heavy_load, number // 4), named(common, number - number // 4 - 1))
    mixed = jax.random.permutation(jax.random.fold_in(own, 3), amount)
    giver, taker = mixed[0:amount // 2 * 2:2], mixed[1:amount // 2 * 2:2]
    slack = jnp.minimum(sizes[giver] - 1, reach - sizes[taker]) // 2
    slack = jnp.where((giver == order[0]) | (taker == order[0]) | (sizes[taker] == 0), 0, jnp.maximum(slack, 0))
    passed = jax.random.randint(jax.random.fold_in(own, 4), (amount // 2,), 0, 1 << 20) % (slack + 1)
    sizes = sizes.at[giver].add(-passed).at[taker].add(passed)
    members = jnp.searchsorted(jnp.cumsum(sizes), jnp.arange(rows * top), side="right").astype(jnp.int32)
    grid = members.reshape(top, rows).T
    grid = grid[jax.random.permutation(jax.random.fold_in(own, 1), rows)]
    offset_by = jax.random.randint(jax.random.fold_in(own, 2), (rows, 1), 0, top)
    return jnp.take_along_axis(grid, (jnp.arange(top)[None, :] + offset_by) % top, axis=1)


def load_shares(amount, total, limit, slope, full):
    loads = [(1 << 20) // math.isqrt(standing ** slope) + 1 for standing in range(1, amount + 1)]
    largest = limit if full else min(limit, max(-(-total // amount), total * loads[0] // sum(loads)))
    least = 1 if total - largest >= amount - 1 else 0
    holding, spare = [largest] + [least] * (amount - 1), total - largest - least * (amount - 1)
    while spare > 0:
        movable = [i for i in range(1, amount) if holding[i] < largest] or [i for i in range(1, amount) if holding[i] < limit]
        whole, left = sum([loads[i] for i in movable]), spare
        for i in movable:
            extra = min(limit - holding[i], max(1, left * loads[i] // whole), spare)
            holding[i] = holding[i] + extra
            spare = spare - extra
    return np.array(holding)


def centred(key, dims, deviation, most, pieces=(), held_as=jnp.bfloat16):
    drawn = jax.random.normal(key, dims, jnp.float32) * deviation
    if len(pieces) > 0:
        drawn = shard_levels(key, dims, pieces, -0.22, 0.18) * drawn
    return jnp.clip(drawn, min=-most, max=most).astype(held_as)


def setup_inputs(seed: int = 0) -> dict:
    splits = jax.random.split(jax.random.key(seed), 16)
    resid = centred(splits[0], (SEQUENCE_TOKENS, D), 1.0, 6.0, ((0, 128),))
    query = centred(splits[1], (SEQUENCE_TOKENS, HEAD_TOTAL * DK), 1.0, 6.0, ((0, 32), (1, 4)))
    forget_logits = draw_forget_logits(jax.random.fold_in(splits[15], 71), 0)
    forget_margin = draw_forget_margin(jax.random.fold_in(splits[15], 71), 0)
    decay_spike = draw_decay_spike(jax.random.fold_in(splits[15], 71), 0)
    value_logits = centred(splits[5], (SEQUENCE_TOKENS, HEAD_TOTAL * DV), 1.0, 6.0, ((0, 32), (1, 4)))
    output_gate_logits = centred(splits[6], (SEQUENCE_TOKENS, HEAD_TOTAL * DV), 1.0, 6.0, ((0, 32), (1, 4)))
    head_norm_scale = jnp.clip(1.0 + 0.18 * jax.random.normal(splits[7], (HEAD_TOTAL * DV,), jnp.float32), 0.1, 1.9)
    output_matrix = centred(splits[8], (HEAD_TOTAL * DV, D), (HEAD_TOTAL * DV) ** -0.5, 0.125)
    norm_scale_vector = jnp.clip(1.0 + 0.18 * jax.random.normal(splits[9], (D,), jnp.float32), 0.1, 1.9)
    routes_keys = jax.random.split(jax.random.fold_in(splits[10], 1), SEQUENCE_TOKENS // ROWS)
    routes_turns = jax.random.permutation(jax.random.fold_in(splits[10], 3), SEQUENCE_TOKENS // ROWS)
    routes = jax.vmap(lambda own, number: shared_out(jax.random.fold_in(splits[10], 2), own, number, ROWS, EXPERTS, TOP, CAP, 2))(routes_keys, routes_turns).reshape((SEQUENCE_TOKENS, TOP))
    routing_weight = jnp.clip(0.2 + 0.8 * jax.random.uniform(splits[11], (SEQUENCE_TOKENS, TOP), jnp.float32) ** shard_levels(splits[11], (SEQUENCE_TOKENS, TOP), ((0, 128),), -0.2, 0.2), 0.2, 1.0)
    gate_matrix = centred(splits[12], (EXPERTS, D, FF), D ** -0.5, 0.125, ((0, 128),))
    up_matrix = centred(splits[13], (EXPERTS, D, FF), D ** -0.5, 0.125, ((0, 128),))
    down_matrix = centred(splits[14], (EXPERTS, FF, D), FF ** -0.5, 0.1875, ((0, 128),))
    return {"resid": resid, "query": query, "forget_logits": forget_logits, "forget_margin": forget_margin, "decay_spike": decay_spike, "value_logits": value_logits, "output_gate_logits": output_gate_logits, "head_norm_scale": head_norm_scale, "output_matrix": output_matrix, "norm_scale_vector": norm_scale_vector, "routes": routes, "routing_weight": routing_weight, "gate_matrix": gate_matrix, "up_matrix": up_matrix, "down_matrix": down_matrix}


maximum_value = lax.Precision.HIGHEST

def to_blocks(matrix, head_number):
    length, columns = matrix.shape
    return matrix.reshape(length // BLOCK, BLOCK, head_number, columns // head_number).transpose(0, 2, 1, 3)

def from_blocks(matrix):
    block_count, head_number, span_len, head_width = matrix.shape
    return matrix.transpose(0, 2, 1, 3).reshape(block_count * span_len, head_number * head_width)

def input_lookup(query, forget_logits, forget_margin, decay_spike, value_logits):
    head_number = decay_spike.shape[1]
    every_key = forget_margin[None, :] * jax.nn.sigmoid(-forget_logits.astype(jnp.float32))
    head_width = every_key.shape[1] // head_number
    logarithm_of_decay = jnp.log1p(-every_key) + jnp.repeat(decay_spike, head_width, axis=1)
    queries = query.astype(jnp.float32) * DK ** (-0.5)
    values = jax.nn.silu(value_logits.astype(jnp.float32))
    return (to_blocks(queries, head_number), to_blocks(every_key, head_number), to_blocks(values, head_number), to_blocks(logarithm_of_decay, head_number))

def block_recurrence(queries, keys_in, values, logarithm_of_decay):
    span_len = queries.shape[2]
    causal = (lax.broadcasted_iota(jnp.int32, (span_len, span_len), 0) >= lax.broadcasted_iota(jnp.int32, (span_len, span_len), 1))[:, :, None]
    cum_log = jnp.cumsum(logarithm_of_decay, axis=2)

    def advance(current_state, inputs):
        query_block, key_b, value_block, cumulative_block = inputs
        spread = cumulative_block[:, :, None, :] - cumulative_block[:, None, :, :]
        weight_t = jnp.where(causal, jnp.exp(jnp.where(causal, spread, 0.0)), 0.0)
        router_scores = jnp.einsum('htk,hsk,htsk->hts', query_block, key_b, weight_t, precision=maximum_value)
        within = jnp.einsum('hts,hsv->htv', router_scores, value_block, precision=maximum_value)
        incoming_state = jnp.einsum('bup,bpl->bul', query_block * jnp.exp(cumulative_block), current_state, precision=maximum_value)
        final_block = cumulative_block[:, -1, :]
        decayed_state = key_b * jnp.exp(final_block[:, None, :] - cumulative_block)
        following_state = jnp.exp(final_block)[:, :, None] * current_state + jnp.einsum('ixq,ixn->iqn', decayed_state, value_block, precision=maximum_value)
        return (following_state, within + incoming_state)
    start_state = jnp.zeros((queries.shape[1], queries.shape[3], values.shape[3]), jnp.float32)
    last_state, outputs = lax.scan(advance, start_state, (queries, keys_in, values, cum_log))
    return (last_state, outputs, cum_log)

def gate_rows(recurrence_output, output_gate_logits, head_norm_scale):
    square = lax.optimization_barrier(jnp.mean(recurrence_output * recurrence_output, axis=3, keepdims=True))
    scaled = from_blocks(recurrence_output * lax.rsqrt(square + 1e-06)) * head_norm_scale[None, :]
    return (scaled * jax.nn.silu(output_gate_logits.astype(jnp.float32))).astype(jnp.bfloat16)

def row_norm(stream, norm_scale_vector):
    values = stream.astype(jnp.float32)
    square = lax.optimization_barrier(jnp.mean(values * values, axis=1, keepdims=True))
    return (values * lax.rsqrt(square + 1e-06) * norm_scale_vector[None, :]).astype(jnp.bfloat16)

def reference(resid, query, forget_logits, forget_margin, decay_spike, value_logits, output_gate_logits, head_norm_scale, output_matrix, norm_scale_vector, routes, routing_weight, gate_matrix, up_matrix, down_matrix):
    block_list = input_lookup(query, forget_logits, forget_margin, decay_spike, value_logits)
    last_state, recurrence_output, cum_log = block_recurrence(*block_list)
    gated_rows = gate_rows(recurrence_output, output_gate_logits, head_norm_scale)
    mixed_rows = jnp.dot(gated_rows, output_matrix, preferred_element_type=jnp.float32)
    stream = (resid.astype(jnp.float32) + mixed_rows).astype(jnp.bfloat16)
    normed = row_norm(stream, norm_scale_vector)
    flat_routes = routes.reshape(-1)
    member = (flat_routes[:, None] == jnp.arange(EXPERTS, dtype=jnp.int32)[None, :]).astype(jnp.int32)
    slot_rank = lax.optimization_barrier(jnp.sum(jnp.cumsum(member, axis=0) * member, axis=1)) - 1
    slot_depth = DEVICES * CAP
    position_entries = (flat_routes * slot_depth + slot_rank).astype(jnp.int32)
    sources = (jnp.arange(flat_routes.shape[0], dtype=jnp.int32) // TOP).astype(jnp.int32)
    buffer = jnp.zeros((EXPERTS * slot_depth, D), jnp.bfloat16).at[position_entries].set(normed[sources])

    def expert_rows(inputs):
        slot_rows, gate_e, up_e, down_e = inputs
        gate_part = jnp.dot(slot_rows, gate_e, preferred_element_type=jnp.float32)
        up_part = jnp.dot(slot_rows, up_e, preferred_element_type=jnp.float32)
        hidden = (jax.nn.silu(gate_part) * up_part).astype(jnp.bfloat16)
        return jnp.dot(hidden, down_e, preferred_element_type=jnp.float32).astype(jnp.bfloat16)
    outputs = lax.map(expert_rows, (buffer.reshape(EXPERTS, slot_depth, D), gate_matrix, up_matrix, down_matrix))
    picked = outputs.reshape(EXPERTS * slot_depth, D)[position_entries].astype(jnp.float32).reshape(-1, TOP, D)
    combined = stream.astype(jnp.float32) + lax.optimization_barrier(jnp.sum(routing_weight[:, :, None] * picked, axis=1))
    return combined.astype(jnp.bfloat16)
```

```python
import functools

import jax
import jax.numpy as jnp
from jax import lax
from jax.experimental import pallas as pl
from jax.experimental.pallas import tpu as pltpu
from jax.sharding import Mesh
from jax.sharding import PartitionSpec as P

DK = 128
BLOCK = 64
SP = ("sp_0", "sp_1", "sp_2")
SP_TP = ("sp_0", "sp_1", "sp_2", "tp")


maximum_value = lax.Precision.HIGHEST


def filled_with(value, identity):
    return jax.tree.map(
        lambda a, e: jnp.broadcast_to(jnp.asarray(e, a.dtype), a.shape), value, identity
    )


def carried_in(value, axes, combine, identity):
    before = start = filled_with(value, identity)
    so_far = value
    for axis in reversed(axes):
        devices, place = (lax.axis_size(axis), lax.axis_index(axis))
        pieces = jax.tree.map(lambda part: lax.all_gather(part, axis), so_far)
        inside, so_far = (start, start)
        for k in range(devices):
            passed = k < place
            so_far = combine(so_far, jax.tree.map(lambda part: part[k], pieces))
            inside = jax.tree.map(lambda new, old: jnp.where(passed, new, old), so_far, inside)
        before = combine(inside, before)
    return before


def in_blocks(value, dim, devices):
    lengths = value.shape
    parts = value.reshape(*lengths[:dim], devices, lengths[dim] // devices, *lengths[dim + 1 :])
    return jnp.moveaxis(parts, dim, 0)


def laid_out(parts, dim):
    parts = jnp.moveaxis(parts, 0, dim)
    lengths = parts.shape
    return parts.reshape(*lengths[:dim], lengths[dim] * lengths[dim + 1], *lengths[dim + 2 :])


def one_exchange(value, axis, axes, splits, concats):
    sizes = [lax.axis_size(a) for a in axes]
    parts = in_blocks(value, splits[0], sizes[0])
    parts = jnp.moveaxis(in_blocks(parts, splits[1] + 1, sizes[1]), 0, 1)
    inside = parts.shape[2:]
    parts = parts.reshape(-1, *inside)
    parts = lax.all_to_all(parts, axis, split_axis=0, concat_axis=0, tiled=True)
    parts = laid_out(parts.reshape(*sizes, *inside), concats[0] + 1)
    return laid_out(parts, concats[1])


def to_blocks(matrix, head_number):
    length, columns = matrix.shape
    return matrix.reshape(length // BLOCK, BLOCK, head_number, columns // head_number).transpose(
        0, 2, 1, 3
    )


def from_blocks(matrix):
    block_count, head_number, span_len, head_width = matrix.shape
    return matrix.transpose(0, 2, 1, 3).reshape(block_count * span_len, head_number * head_width)


def input_lookup(query, forget_logits, forget_margin, decay_spike, value_logits):
    head_number = decay_spike.shape[1]
    every_key = forget_margin[None, :] * jax.nn.sigmoid(-forget_logits.astype(jnp.float32))
    head_width = every_key.shape[1] // head_number
    logarithm_of_decay = jnp.log1p(-every_key) + jnp.repeat(decay_spike, head_width, axis=1)
    queries = query.astype(jnp.float32) * DK ** (-0.5)
    values = jax.nn.silu(value_logits.astype(jnp.float32))
    return (
        to_blocks(queries, head_number),
        to_blocks(every_key, head_number),
        to_blocks(values, head_number),
        to_blocks(logarithm_of_decay, head_number),
    )


def block_recurrence(queries, keys_in, values, logarithm_of_decay):
    span_len = queries.shape[2]
    causal = (
        lax.broadcasted_iota(jnp.int32, (span_len, span_len), 0)
        >= lax.broadcasted_iota(jnp.int32, (span_len, span_len), 1)
    )[:, :, None]
    cum_log = jnp.cumsum(logarithm_of_decay, axis=2)

    def advance(current_state, inputs):
        query_block, key_b, value_block, cumulative_block = inputs
        spread = cumulative_block[:, :, None, :] - cumulative_block[:, None, :, :]
        weight_t = jnp.where(causal, jnp.exp(jnp.where(causal, spread, 0.0)), 0.0)
        router_scores = jnp.einsum(
            "htk,hsk,htsk->hts", query_block, key_b, weight_t, precision=maximum_value
        )
        within = jnp.einsum("hts,hsv->htv", router_scores, value_block, precision=maximum_value)
        incoming_state = jnp.einsum(
            "bup,bpl->bul",
            query_block * jnp.exp(cumulative_block),
            current_state,
            precision=maximum_value,
        )
        final_block = cumulative_block[:, -1, :]
        decayed_state = key_b * jnp.exp(final_block[:, None, :] - cumulative_block)
        following_state = jnp.exp(final_block)[:, :, None] * current_state + jnp.einsum(
            "ixq,ixn->iqn", decayed_state, value_block, precision=maximum_value
        )
        return (following_state, within + incoming_state)

    start_state = jnp.zeros((queries.shape[1], queries.shape[3], values.shape[3]), jnp.float32)
    last_state, outputs = lax.scan(advance, start_state, (queries, keys_in, values, cum_log))
    return (last_state, outputs, cum_log)


def gate_rows(recurrence_output, output_gate_logits, head_norm_scale):
    square = jnp.mean(recurrence_output * recurrence_output, axis=3, keepdims=True)
    scaled = from_blocks(recurrence_output * lax.rsqrt(square + 1e-06)) * head_norm_scale[None, :]
    return (scaled * jax.nn.silu(output_gate_logits.astype(jnp.float32))).astype(jnp.bfloat16)


def row_norm(stream, norm_scale_vector):
    values = stream.astype(jnp.float32)
    square = jnp.mean(values * values, axis=1, keepdims=True)
    return (values * lax.rsqrt(square + 1e-06) * norm_scale_vector[None, :]).astype(jnp.bfloat16)


def join_states(earlier, later):
    early_log, early_state = earlier
    late_log, late_state = later
    return (early_log + late_log, jnp.exp(late_log)[:, :, None] * early_state + late_state)


def expert_block(slot_rows, gate_matrix, up_matrix, down_matrix):
    gate_part = jnp.einsum(
        "...ecd,edf->...ecf", slot_rows, gate_matrix, preferred_element_type=jnp.float32
    )
    up_part = jnp.einsum(
        "...ecd,edf->...ecf", slot_rows, up_matrix, preferred_element_type=jnp.float32
    )
    hidden = (jax.nn.silu(gate_part) * up_part).astype(jnp.bfloat16)
    return jnp.einsum(
        "...ecf,efd->...ecd", hidden, down_matrix, preferred_element_type=jnp.float32
    ).astype(jnp.bfloat16)


MESH = pl.DeviceIdType.MESH
F32 = jnp.float32
BF16 = jnp.bfloat16
I32 = jnp.int32
GROUPS = 4
PER = 32


def coords():
    sp = lax.axis_index("sp")
    return sp // 8, (sp // 2) % 4, sp % 2, lax.axis_index("tp")


def peer(d, sign):
    z, y, c, x = coords()
    g, j = d // PER, d % PER
    dz, dy, dc = j // 8, (j // 2) % 4, j % 2
    dx = (g + 8 - dz - dy) % 4
    if sign < 0:
        dz, dy, dx = 4 - dz, 4 - dy, 4 - dx
    z, y, c, x = (z + dz) % 4, (y + dy) % 4, (c + dc) % 2, (x + dx) % 4
    return ((z * 4 + y) * 2 + c, x)


def entry_barrier():
    barrier = pltpu.get_barrier_semaphore()

    @pl.loop(1, GROUPS * PER)
    def _(d):
        pl.semaphore_signal(barrier, inc=1, device_id=peer(d, 1), device_id_type=MESH)

    return barrier


def iota(shape, dim):
    return lax.broadcasted_iota(I32, shape, dim)


def slot_tables(routes, weights, pack_l, comb_l):
    z, y, c, x = coords()
    d = iota((128, 128), 0)
    dz, dy, dc = (d >> 3) & 3, (d >> 1) & 3, d & 1
    dx = ((d >> 5) + 8 - dz - dy) & 3
    expert = (((((z + dz) & 3) * 4 + ((y + dy) & 3)) * 2 + ((c + dc) & 1)) * 4) + ((x + dx) & 3)
    first = routes[0:1, :] == expert
    second = routes[1:2, :] == expert
    member = jnp.where(first, 1.0, jnp.where(second, 1.0, 0.0))
    earlier = jnp.where(iota((128, 128), 0) < iota((128, 128), 1), 1.0, 0.0).astype(BF16)
    rank = jnp.dot(member.astype(BF16), earlier, preferred_element_type=F32)
    code = (member * (rank + 1.0)).astype(BF16)
    share = jnp.where(first, weights[0:1, :], jnp.where(second, weights[1:2, :], 0.0))
    high = share.astype(BF16)
    low = (share - high.astype(F32)).astype(BF16)
    table = jnp.concatenate([code, high, low], axis=1)
    rows = PER * 8
    at = iota((rows, 128), 0)
    wanted = ((at & 3) + 1).astype(F32)
    upper = ((at >> 2) & 1) == 0
    for g in range(GROUPS):
        spread = jnp.where((at >> 3) + g * PER == iota((rows, 128), 1), 1.0, 0.0).astype(BF16)
        wide = jnp.dot(spread, table, preferred_element_type=F32)
        chosen = wide[:, :128] == wanted
        one = jnp.where(chosen, 1.0, 0.0)
        high_g = jnp.where(chosen, wide[:, 128:256], 0.0)
        low_g = jnp.where(chosen, wide[:, 256:], 0.0)
        zero = jnp.zeros_like(one)
        pack_l[g] = jnp.concatenate(
            [jnp.where(upper, one, zero), jnp.where(upper, zero, one)], axis=1
        ).astype(BF16)
        comb_l[g] = jnp.concatenate(
            [
                jnp.where(upper, high_g, zero),
                jnp.where(upper, zero, high_g),
                jnp.where(upper, low_g, zero),
                jnp.where(upper, zero, low_g),
            ],
            axis=1,
        ).astype(BF16)


def blocks(ref, lo, count):
    return ref.at[pl.ds(lo, count)]


def wait_group(buf, sem, g):
    z, y, c, x = coords()
    other = (lax.axis_index("sp"), (x + 1) % 4)

    @pl.when(g == 0)
    def _():
        part = blocks(buf, 1, PER - 1)
        pltpu.make_async_remote_copy(part, part, sem, sem, other, MESH).wait_recv()

    @pl.when(g > 0)
    def _():
        part = blocks(buf, g * PER, PER)
        pltpu.make_async_remote_copy(part, part, sem, sem, other, MESH).wait_recv()


def send_group(src, dst, send_sem, recv_sem, g, sign):
    @pl.loop(0, PER)
    def _(j):
        d = g * PER + j

        @pl.when(d > 0)
        def _():
            pltpu.make_async_remote_copy(
                src.at[d], dst.at[d], send_sem, recv_sem, peer(d, sign), MESH
            ).start()


def wait_sent(buf, sem):
    x = lax.axis_index("tp")
    part = blocks(buf, 1, GROUPS * PER - 1)
    pltpu.make_async_remote_copy(
        part, part, sem, sem, (lax.axis_index("sp"), (x + 1) % 4), MESH
    ).wait_send()


def expert_phase(stream, normed, pack_l, comb_l, gate, up, down, weight_copies, bufs, total, out):
    out_slots, in_slots, answers, replies, send_sem, recv_sem, send_back, recv_back = bufs
    halves = jnp.concatenate([normed[:, :1024], normed[:, 1024:]], axis=0)
    for g in range(GROUPS):
        packed = jnp.dot(pack_l[g], halves, preferred_element_type=F32).astype(BF16)
        out_slots[pl.ds(g * PER, PER)] = packed.reshape(PER, 8, 1024)
        send_group(out_slots, in_slots, send_sem, recv_sem.at[g], g, 1)
    in_slots[0] = out_slots[0]
    for copy in weight_copies:
        copy.wait()
    rows = PER * 8
    a, b = iota((rows, rows), 0), iota((rows, rows), 1)
    place = ((a & 127) >> 2) * 8 + (a >> 7) * 4 + (a & 3)
    unpack = jnp.where(place == b, 1.0, 0.0).astype(BF16)
    place_b = ((b & 127) >> 2) * 8 + (b >> 7) * 4 + (b & 3)
    repack = jnp.where(place_b == a, 1.0, 0.0).astype(BF16)

    @pl.loop(0, GROUPS)
    def _(g):
        wait_group(in_slots, recv_sem.at[g], g)
        came = in_slots[pl.ds(g * PER, PER)].reshape(rows, 1024)
        flat = jnp.dot(unpack, came, preferred_element_type=F32).astype(BF16)
        x = jnp.concatenate([flat[:128], flat[128:]], axis=1)
        hidden = []
        for n in range(0, 1024, 256):
            gated = jnp.dot(x, gate[:, n : n + 256], preferred_element_type=F32)
            lifted = jnp.dot(x, up[:, n : n + 256], preferred_element_type=F32)
            hidden.append((gated * jax.nn.sigmoid(gated) * lifted).astype(BF16))
        hidden = jnp.concatenate(hidden, axis=1)
        y0 = jnp.dot(hidden, down[:, :1024], preferred_element_type=F32).astype(BF16)
        y1 = jnp.dot(hidden, down[:, 1024:], preferred_element_type=F32).astype(BF16)
        both = jnp.concatenate([y0, y1], axis=0)
        back = jnp.dot(repack, both, preferred_element_type=F32).astype(BF16)
        answers[pl.ds(g * PER, PER)] = back.reshape(PER, 8, 1024)
        send_group(answers, replies, send_back, recv_back.at[g], g, -1)

    replies[0] = answers[0]
    total[...] = jnp.zeros_like(total)

    @pl.loop(0, GROUPS)
    def _(g):
        wait_group(replies, recv_back.at[g], g)
        got = replies[pl.ds(g * PER, PER)].reshape(rows, 1024)
        total[...] += lax.dot_general(
            comb_l[g], got, (((0,), (0,)), ((), ())), preferred_element_type=F32
        )

    for h in range(2):
        part = total[h * 128 : h * 128 + 128] + total[256 + h * 128 : 256 + h * 128 + 128]
        cols = slice(h * 1024, h * 1024 + 1024)
        out[:, cols] = (stream[:, cols].astype(F32) + part).astype(BF16)
    wait_sent(out_slots, send_sem)
    wait_sent(answers, send_back)


def slot_buffers():
    slots = pltpu.VMEM((GROUPS * PER, 8, 1024), BF16)
    dma = pltpu.SemaphoreType.DMA
    return [slots] * 4 + [dma, dma((GROUPS,)), dma, dma((GROUPS,))]


def expert_kernel(
    stream, scale, routes, weights, gate_hbm, up_hbm, down_hbm, out,
    gate, up, down, w_sems, pack_l, comb_l, total, *bufs,
):
    barrier = entry_barrier()
    copies = [
        pltpu.make_async_copy(src.at[0], dst, w_sems.at[i])
        for i, (src, dst) in enumerate(((gate_hbm, gate), (up_hbm, up), (down_hbm, down)))
    ]
    for copy in copies:
        copy.start()
    slot_tables(routes, weights, pack_l, comb_l)
    values = stream[...].astype(F32)
    square = jnp.mean(values * values, axis=1, keepdims=True)
    normed = (values * lax.rsqrt(square + 1e-06) * scale[...]).astype(BF16)
    pl.semaphore_wait(barrier, GROUPS * PER - 1)
    expert_phase(stream, normed, pack_l, comb_l, gate, up, down, copies, bufs, total, out)


def expert_call(stream, scale, routes, weights, gate, up, down):
    vmem = pl.BlockSpec(memory_space=pltpu.VMEM)
    hbm = pl.BlockSpec(memory_space=pl.ANY)
    return pl.pallas_call(
        expert_kernel,
        out_shape=jax.ShapeDtypeStruct((128, 2048), BF16),
        in_specs=[vmem] * 4 + [hbm] * 3,
        out_specs=vmem,
        scratch_shapes=[
            pltpu.VMEM((2048, 1024), BF16),
            pltpu.VMEM((2048, 1024), BF16),
            pltpu.VMEM((1024, 2048), BF16),
            pltpu.SemaphoreType.DMA((3,)),
            pltpu.VMEM((GROUPS, PER * 8, 256), BF16),
            pltpu.VMEM((GROUPS, PER * 8, 512), BF16),
            pltpu.VMEM((512, 1024), F32),
        ]
        + slot_buffers(),
        compiler_params=pltpu.CompilerParams(
            collective_id=0, has_side_effects=True, vmem_limit_bytes=60 * 1024 * 1024
        ),
    )(stream, scale.reshape(1, 2048), routes.T, weights.T, gate, up, down)


def body(
    resid,
    query,
    forget_logits,
    forget_margin,
    decay_spike,
    value_logits,
    output_gate_logits,
    head_norm_scale,
    output_matrix,
    norm_scale_vector,
    routes,
    routing_weight,
    gate_matrix,
    up_matrix,
    down_matrix,
):
    queries, keys_b, values, logarithm_of_decay = input_lookup(
        query, forget_logits, forget_margin, decay_spike, value_logits
    )
    last_state, recurrence_output, cum_log = block_recurrence(
        queries, keys_b, values, logarithm_of_decay
    )
    totals = cum_log[:, :, -1, :]
    before = jnp.cumsum(totals, axis=0) - totals
    device_log = jnp.sum(totals, axis=0)
    identity = (jnp.zeros_like(device_log), jnp.zeros_like(last_state))
    prior_state = carried_in((device_log, last_state), SP, join_states, identity)[1]
    readout_result = queries * jnp.exp(cum_log + before[:, :, None, :])
    recurrence_output = recurrence_output + jnp.einsum(
        "gwme,wej->gwmj", readout_result, prior_state, precision=maximum_value
    )
    gated_rows = gate_rows(recurrence_output, output_gate_logits, head_norm_scale)
    arrived_rows = lax.all_to_all(gated_rows, "tp", split_axis=0, concat_axis=1, tiled=True)
    mixed_rows = jnp.dot(arrived_rows, output_matrix, preferred_element_type=jnp.float32)
    stream = (resid.astype(jnp.float32) + mixed_rows).astype(jnp.bfloat16)
    return stream


def solution(mesh):
    finer = Mesh(mesh.devices.reshape(4, 4, 2, mesh.shape["tp"]), ("sp_0", "sp_1", "sp_2", "tp"))
    placed = (
        P(SP_TP, None),
        P(SP, "tp"),
        P(SP, "tp"),
        P("tp"),
        P(SP, "tp"),
        P(SP, "tp"),
        P(SP, "tp"),
        P("tp"),
        P(),
        P(),
        P(SP_TP, None),
        P(SP_TP, None),
        P(SP_TP, None, None),
        P(SP_TP, None, None),
        P(SP_TP, None, None),
    )
    front = jax.shard_map(
        body, mesh=finer, in_specs=placed, out_specs=P(SP_TP, None), check_vma=False
    )
    whole = ("sp", "tp")
    back = jax.shard_map(
        expert_call,
        mesh=mesh,
        in_specs=(P(whole, None), P(), P(whole, None), P(whole, None)) + (P(whole, None, None),) * 3,
        out_specs=P(whole, None),
        check_vma=False,
    )

    def run(*args):
        return back(front(*args), args[9], *args[10:])

    return run
```

```python
import jax
import jax.numpy as jnp
from jax import lax
from jax.experimental import pallas as pl
from jax.experimental.pallas import tpu as pltpu
from jax.sharding import PartitionSpec as P

MESH = pl.DeviceIdType.MESH
F32 = jnp.float32
BF16 = jnp.bfloat16
I32 = jnp.int32
GROUPS = 4
PER = 32


def coords():
    sp = lax.axis_index("sp")
    return sp // 8, (sp // 2) % 4, sp % 2, lax.axis_index("tp")


def peer(d, sign):
    z, y, c, x = coords()
    g, j = d // PER, d % PER
    dz, dy, dc = j // 8, (j // 2) % 4, j % 2
    dx = (g + 8 - dz - dy) % 4
    if sign < 0:
        dz, dy, dx = 4 - dz, 4 - dy, 4 - dx
    z, y, c, x = (z + dz) % 4, (y + dy) % 4, (c + dc) % 2, (x + dx) % 4
    return ((z * 4 + y) * 2 + c, x)


def entry_barrier():
    barrier = pltpu.get_barrier_semaphore()

    @pl.loop(1, GROUPS * PER)
    def _(d):
        pl.semaphore_signal(barrier, inc=1, device_id=peer(d, 1), device_id_type=MESH)

    return barrier


def iota(shape, dim):
    return lax.broadcasted_iota(I32, shape, dim)


def slot_tables(routes, weights, pack_l, comb_l):
    z, y, c, x = coords()
    d = iota((128, 128), 0)
    dz, dy, dc = (d >> 3) & 3, (d >> 1) & 3, d & 1
    dx = ((d >> 5) + 8 - dz - dy) & 3
    expert = (((((z + dz) & 3) * 4 + ((y + dy) & 3)) * 2 + ((c + dc) & 1)) * 4) + ((x + dx) & 3)
    first = routes[0:1, :] == expert
    second = routes[1:2, :] == expert
    member = jnp.where(first, 1.0, jnp.where(second, 1.0, 0.0))
    earlier = jnp.where(iota((128, 128), 0) < iota((128, 128), 1), 1.0, 0.0).astype(BF16)
    rank = jnp.dot(member.astype(BF16), earlier, preferred_element_type=F32)
    code = (member * (rank + 1.0)).astype(BF16)
    share = jnp.where(first, weights[0:1, :], jnp.where(second, weights[1:2, :], 0.0))
    high = share.astype(BF16)
    low = (share - high.astype(F32)).astype(BF16)
    table = jnp.concatenate([code, high, low], axis=1)
    rows = PER * 8
    at = iota((rows, 128), 0)
    wanted = ((at & 3) + 1).astype(F32)
    upper = ((at >> 2) & 1) == 0
    for g in range(GROUPS):
        spread = jnp.where((at >> 3) + g * PER == iota((rows, 128), 1), 1.0, 0.0).astype(BF16)
        wide = jnp.dot(spread, table, preferred_element_type=F32)
        chosen = wide[:, :128] == wanted
        one = jnp.where(chosen, 1.0, 0.0)
        high_g = jnp.where(chosen, wide[:, 128:256], 0.0)
        low_g = jnp.where(chosen, wide[:, 256:], 0.0)
        zero = jnp.zeros_like(one)
        pack_l[g] = jnp.concatenate(
            [jnp.where(upper, one, zero), jnp.where(upper, zero, one)], axis=1
        ).astype(BF16)
        comb_l[g] = jnp.concatenate(
            [
                jnp.where(upper, high_g, zero),
                jnp.where(upper, zero, high_g),
                jnp.where(upper, low_g, zero),
                jnp.where(upper, zero, low_g),
            ],
            axis=1,
        ).astype(BF16)


def blocks(ref, lo, count):
    return ref.at[pl.ds(lo, count)]


def wait_group(buf, sem, g):
    z, y, c, x = coords()
    other = (lax.axis_index("sp"), (x + 1) % 4)

    @pl.when(g == 0)
    def _():
        part = blocks(buf, 1, PER - 1)
        pltpu.make_async_remote_copy(part, part, sem, sem, other, MESH).wait_recv()

    @pl.when(g > 0)
    def _():
        part = blocks(buf, g * PER, PER)
        pltpu.make_async_remote_copy(part, part, sem, sem, other, MESH).wait_recv()


def send_group(src, dst, send_sem, recv_sem, g, sign):
    @pl.loop(0, PER)
    def _(j):
        d = g * PER + j

        @pl.when(d > 0)
        def _():
            pltpu.make_async_remote_copy(
                src.at[d], dst.at[d], send_sem, recv_sem, peer(d, sign), MESH
            ).start()


def wait_sent(buf, sem):
    x = lax.axis_index("tp")
    part = blocks(buf, 1, GROUPS * PER - 1)
    pltpu.make_async_remote_copy(
        part, part, sem, sem, (lax.axis_index("sp"), (x + 1) % 4), MESH
    ).wait_send()


def expert_phase(stream, normed, pack_l, comb_l, gate, up, down, weight_copies, bufs, total, out):
    out_slots, in_slots, answers, replies, send_sem, recv_sem, send_back, recv_back = bufs
    halves = jnp.concatenate([normed[:, :1024], normed[:, 1024:]], axis=0)
    for g in range(GROUPS):
        with jax.named_scope("pack"):
            packed = jnp.dot(pack_l[g], halves, preferred_element_type=F32).astype(BF16)
            out_slots[pl.ds(g * PER, PER)] = packed.reshape(PER, 8, 1024)
        with jax.named_scope("dispatch"):
            send_group(out_slots, in_slots, send_sem, recv_sem.at[g], g, 1)
    in_slots[0] = out_slots[0]
    for copy in weight_copies:
        copy.wait()
    rows = PER * 8
    a, b = iota((rows, rows), 0), iota((rows, rows), 1)
    place = ((a & 127) >> 2) * 8 + (a >> 7) * 4 + (a & 3)
    unpack = jnp.where(place == b, 1.0, 0.0).astype(BF16)
    place_b = ((b & 127) >> 2) * 8 + (b >> 7) * 4 + (b & 3)
    repack = jnp.where(place_b == a, 1.0, 0.0).astype(BF16)

    @pl.loop(0, GROUPS)
    def _(g):
        with jax.named_scope("slots_wait"):
            wait_group(in_slots, recv_sem.at[g], g)
        came = in_slots[pl.ds(g * PER, PER)].reshape(rows, 1024)
        flat = jnp.dot(unpack, came, preferred_element_type=F32).astype(BF16)
        x = jnp.concatenate([flat[:128], flat[128:]], axis=1)
        hidden = []
        for n in range(0, 1024, 256):
            gated = jnp.dot(x, gate[:, n : n + 256], preferred_element_type=F32)
            lifted = jnp.dot(x, up[:, n : n + 256], preferred_element_type=F32)
            hidden.append((gated * jax.nn.sigmoid(gated) * lifted).astype(BF16))
        hidden = jnp.concatenate(hidden, axis=1)
        y0 = jnp.dot(hidden, down[:, :1024], preferred_element_type=F32).astype(BF16)
        y1 = jnp.dot(hidden, down[:, 1024:], preferred_element_type=F32).astype(BF16)
        both = jnp.concatenate([y0, y1], axis=0)
        back = jnp.dot(repack, both, preferred_element_type=F32).astype(BF16)
        answers[pl.ds(g * PER, PER)] = back.reshape(PER, 8, 1024)
        with jax.named_scope("answer_send"):
            send_group(answers, replies, send_back, recv_back.at[g], g, -1)

    replies[0] = answers[0]
    total[...] = jnp.zeros_like(total)

    @pl.loop(0, GROUPS)
    def _(g):
        with jax.named_scope("replies_wait"):
            wait_group(replies, recv_back.at[g], g)
        got = replies[pl.ds(g * PER, PER)].reshape(rows, 1024)
        total[...] += lax.dot_general(
            comb_l[g], got, (((0,), (0,)), ((), ())), preferred_element_type=F32
        )

    for h in range(2):
        part = total[h * 128 : h * 128 + 128] + total[256 + h * 128 : 256 + h * 128 + 128]
        cols = slice(h * 1024, h * 1024 + 1024)
        out[:, cols] = (stream[:, cols].astype(F32) + part).astype(BF16)
    wait_sent(out_slots, send_sem)
    wait_sent(answers, send_back)


def slot_buffers():
    slots = pltpu.VMEM((GROUPS * PER, 8, 1024), BF16)
    dma = pltpu.SemaphoreType.DMA
    return [slots] * 4 + [dma, dma((GROUPS,)), dma, dma((GROUPS,))]


def sp_peer(i):
    return (i, lax.axis_index("tp"))


def tp_peer(i):
    return (lax.axis_index("sp"), i)


def dot_nt(a, b):
    return lax.dot_general(a, b, (((1,), (1,)), ((), ())), preferred_element_type=F32)


def dot_tn(a, b):
    return lax.dot_general(a, b, (((0,), (0,)), ((), ())), preferred_element_type=F32)


def dot(a, b):
    return jnp.dot(a, b, preferred_element_type=F32)


def split(value):
    high = value.astype(BF16)
    return high, (value - high.astype(F32)).astype(BF16)


def spike_sums(spikes, run_row, run_col):
    at_or_before = jnp.where(iota((512, 512), 0) <= iota((512, 512), 1), 1.0, 0.0).astype(BF16)
    after = jnp.where(iota((512, 512), 0) >= iota((512, 512), 1), 1.0, 0.0).astype(BF16)
    rest = spikes[...]
    row, col = jnp.zeros((8, 512), F32), jnp.zeros((512, 8), F32)
    for _ in range(3):
        part = rest.astype(BF16)
        rest = rest - part.astype(F32)
        row = row + dot(part, at_or_before)
        col = col + dot_nt(after, part)
    run_row[...] = row
    run_col[...] = col


def channel_pass(query, forget, value, margin, qd, kd, vv, last):
    lower = jnp.where(iota((128, 128), 0) >= iota((128, 128), 1), 1.0, 0.0).astype(BF16)
    last[...] = jnp.zeros_like(last)

    @pl.loop(0, 4)
    def _(b):
        rows = pl.ds(pl.multiple_of(b * 128, 128), 128)
        for n in range(0, 512, 128):
            cols = slice(n, n + 128)
            keys = margin[:, cols] * jax.nn.sigmoid(-forget[rows, cols].astype(F32))
            high, low = split(jnp.log1p(-keys))
            run = dot(lower, high) + dot(lower, low) + last[:, cols]
            last[:, cols] = run[127:128]
            kd[rows, cols] = (keys * jnp.exp(-run)).astype(BF16)
            qd[rows, cols] = (query[rows, cols].astype(F32) * jnp.exp(run) * 128**-0.5).astype(BF16)
            logits = value[rows, cols].astype(F32)
            vv[rows, cols] = (logits * jax.nn.sigmoid(logits)).astype(BF16)


def own_states(kd, vv, last, run_row, run_col, state_out, decay_out):
    for h in range(4):
        cols = slice(h * 128, h * 128 + 128)
        total = run_row[h : h + 1, 511:512]
        fade = jnp.exp(total - run_col[:, h : h + 1])
        keys = (kd[:, cols].astype(F32) * fade).astype(BF16)
        state = dot_tn(vv[:, cols], keys) * jnp.exp(last[:, cols])
        state_out[pl.ds(h * 8, 8)] = state.astype(BF16).reshape(8, 16, 128)
        decay_out[h] = last[:, cols] + total


def within_pass(qd, kd, vv, run_row, run_col, local):
    causal = iota((128, 128), 0) >= iota((128, 128), 1)
    for h in range(4):
        cols = slice(h * 128, h * 128 + 128)
        for i in range(4):
            rows = slice(i * 128, i * 128 + 128)
            seen = (i + 1) * 128
            scores = dot_nt(qd[rows, cols], kd[:seen, cols])
            gap = run_col[rows, h : h + 1] - run_row[h : h + 1, :seen]
            edge = slice(i * 128, seen)
            inner = jnp.where(causal, scores[:, edge] * jnp.exp(jnp.where(causal, gap[:, edge], 0.0)), 0.0)
            parts = [inner.astype(BF16)]
            if i:
                parts.insert(0, (scores[:, : i * 128] * jnp.exp(gap[:, : i * 128])).astype(BF16))
            weights = jnp.concatenate(parts, axis=1)
            local[rows, cols] = dot(weights, vv[:seen, cols])


def send_states(state_out, decay_out, state_in, decay_in, sems):
    me = lax.axis_index("sp")
    send, recv, send_d, recv_d = sems

    @pl.loop(1, 32)
    def _(d):
        p = (me + d) % 32
        pltpu.make_async_remote_copy(
            decay_out.at[p // 8], decay_in.at[me], send_d, recv_d, sp_peer(p), MESH
        ).start()
        pltpu.make_async_remote_copy(
            state_out.at[p], state_in.at[me], send, recv, sp_peer(p), MESH
        ).start()

    state_in[me] = state_out[me]
    decay_in[me] = decay_out[me // 8]


def wait_bytes(part, sem, sent):
    copy = pltpu.make_async_remote_copy(
        part, part, sem, sem, tp_peer((lax.axis_index("tp") + 1) % 4), MESH
    )
    if sent:
        copy.wait_send()
    else:
        copy.wait_recv()


def scan_states(state_in, decay_in, prior_out, prior_in, sems, back):
    send, recv, send_d, recv_d = sems
    wait_bytes(state_in.at[pl.ds(0, 31)], recv, False)
    wait_bytes(decay_in.at[pl.ds(0, 31)], recv_d, False)
    state = jnp.zeros((16, 128), F32)
    for i in range(32):
        prior_out[i] = state.astype(BF16)
        state = jnp.exp(decay_in[i]) * state + state_in[i].astype(F32)
    me = lax.axis_index("sp")

    @pl.loop(1, 32)
    def _(d):
        p = (me + d) % 32
        pltpu.make_async_remote_copy(
            prior_out.at[p], prior_in.at[me], back[0], back[1], sp_peer(p), MESH
        ).start()

    prior_in[me] = prior_out[me]


def gate_pass(qd, run_col, local, prior_in, out_gate, head_scale, gated_out, gated_in, sems):
    x = lax.axis_index("tp")

    def block(j):
        rows = pl.ds(pl.multiple_of(j * 128, 128), 128)
        for h in range(4):
            cols = slice(h * 128, h * 128 + 128)
            asked = (qd[rows, cols].astype(F32) * jnp.exp(run_col[rows, h : h + 1])).astype(BF16)
            prior = prior_in[pl.ds(h * 8, 8)].reshape(128, 128)
            full = local[rows, cols] + dot_nt(asked, prior)
            square = jnp.mean(full * full, axis=1, keepdims=True)
            logits = out_gate[rows, cols].astype(F32)
            done = full * lax.rsqrt(square + 1e-06) * head_scale[:, cols] * (logits * jax.nn.sigmoid(logits))
            gated_out[j, :, cols] = done.astype(BF16)

    @pl.loop(0, 4)
    def _(k):
        j = (x + 2 + k) % 4
        j = jnp.where(k == 0, (x + 2) % 4, jnp.where(k == 1, (x + 1) % 4, jnp.where(k == 2, (x + 3) % 4, x)))
        block(j)

        @pl.when(k < 3)
        def _():
            pltpu.make_async_remote_copy(
                gated_out.at[j], gated_in.at[x], sems[0], sems[1].at[k], tp_peer(j), MESH
            ).start()

    gated_in[x] = gated_out[x]


def project(gated_in, matrix, mixed, sems):
    x = lax.axis_index("tp")
    mixed[...] = dot(gated_in[x], matrix[pl.ds(pl.multiple_of(x * 512, 512), 512)])
    for k, back in ((1, 3), (2, 1), (0, 2)):
        i = (x + back) % 4
        wait_bytes(gated_in.at[i], sems[1].at[k], False)
        mixed[...] += dot(gated_in[i], matrix[pl.ds(pl.multiple_of(i * 512, 512), 512)])


def layer_kernel(
    resid_hbm, query_hbm, forget_hbm, margin, spikes, value_hbm, gate_logits_hbm, head_scale,
    matrix_hbm, scale, routes, weights, gate_hbm, up_hbm, down_hbm, out,
    resid, query, forget, value, gate_logits, matrix, gate, up, down, in_sems,
    qd, kd, vv, last, run_row, run_col, local, mixed, pack_l, comb_l, total,
    state_out, state_in, prior_out, prior_in, decay_out, decay_in, gated_out, gated_in,
    state_send, state_recv, decay_send, decay_recv, prior_send, prior_recv, gated_send, gated_recv,
    *bufs,
):
    moves = [
        (forget_hbm, forget), (query_hbm, query), (value_hbm, value), (gate_logits_hbm, gate_logits),
        (resid_hbm, resid), (matrix_hbm, matrix), (gate_hbm.at[0], gate), (up_hbm.at[0], up),
        (down_hbm.at[0], down),
    ]
    copies = [pltpu.make_async_copy(src, dst, in_sems.at[i]) for i, (src, dst) in enumerate(moves)]
    for copy in copies:
        copy.start()
    with jax.named_scope("greet"):
        barrier = entry_barrier()
    with jax.named_scope("spikes"):
        spike_sums(spikes, run_row, run_col)
    with jax.named_scope("inputs"):
        for copy in copies[:3]:
            copy.wait()
    with jax.named_scope("channels"):
        channel_pass(query, forget, value, margin, qd, kd, vv, last)
    with jax.named_scope("states"):
        own_states(kd, vv, last, run_row, run_col, state_out, decay_out)
    with jax.named_scope("met"):
        pl.semaphore_wait(barrier, GROUPS * PER - 1)
    sems = (state_send, state_recv, decay_send, decay_recv)
    with jax.named_scope("state_send"):
        send_states(state_out, decay_out, state_in, decay_in, sems)
    with jax.named_scope("within"):
        within_pass(qd, kd, vv, run_row, run_col, local)
    back = (prior_send, prior_recv)
    with jax.named_scope("scan"):
        scan_states(state_in, decay_in, prior_out, prior_in, sems, back)
    with jax.named_scope("tables"):
        slot_tables(routes, weights, pack_l, comb_l)
    copies[3].wait()
    with jax.named_scope("prior_wait"):
        wait_bytes(prior_in.at[pl.ds(0, 31)], prior_recv, False)
    gated = (gated_send, gated_recv)
    with jax.named_scope("gating"):
        gate_pass(qd, run_col, local, prior_in, gate_logits, head_scale, gated_out, gated_in, gated)
    copies[4].wait()
    copies[5].wait()
    with jax.named_scope("project"):
        project(gated_in, matrix, mixed, gated)
    stream = (resid[...].astype(F32) + mixed[...]).astype(BF16)
    resid[...] = stream
    values = stream.astype(F32)
    square = jnp.mean(values * values, axis=1, keepdims=True)
    normed = (values * lax.rsqrt(square + 1e-06) * scale[...]).astype(BF16)
    with jax.named_scope("experts"):
        expert_phase(resid, normed, pack_l, comb_l, gate, up, down, copies[6:], bufs, total, out)
    wait_bytes(state_out.at[pl.ds(0, 31)], state_send, True)
    wait_bytes(decay_in.at[pl.ds(0, 31)], decay_send, True)
    wait_bytes(prior_out.at[pl.ds(0, 31)], prior_send, True)
    wait_bytes(gated_out.at[pl.ds(0, 3)], gated_send, True)


def layer(
    resid, query, forget_logits, forget_margin, decay_spike, value_logits, output_gate_logits,
    head_norm_scale, output_matrix, norm_scale_vector, routes, routing_weight, gate, up, down,
):
    vmem = pl.BlockSpec(memory_space=pltpu.VMEM)
    hbm = pl.BlockSpec(memory_space=pl.ANY)
    dma = pltpu.SemaphoreType.DMA
    wide = pltpu.VMEM((512, 512), BF16)
    pieces = pltpu.VMEM((32, 16, 128), BF16)
    return pl.pallas_call(
        layer_kernel,
        out_shape=jax.ShapeDtypeStruct((128, 2048), BF16),
        in_specs=[hbm, hbm, hbm, vmem, vmem, hbm, hbm, vmem, hbm, vmem, vmem, vmem, hbm, hbm, hbm],
        out_specs=vmem,
        scratch_shapes=[
            pltpu.VMEM((128, 2048), BF16),
            wide,
            wide,
            wide,
            wide,
            pltpu.VMEM((2048, 2048), BF16),
            pltpu.VMEM((2048, 1024), BF16),
            pltpu.VMEM((2048, 1024), BF16),
            pltpu.VMEM((1024, 2048), BF16),
            dma((9,)),
            wide,
            wide,
            wide,
            pltpu.VMEM((1, 512), F32),
            pltpu.VMEM((8, 512), F32),
            pltpu.VMEM((512, 8), F32),
            pltpu.VMEM((512, 512), F32),
            pltpu.VMEM((128, 2048), F32),
            pltpu.VMEM((GROUPS, PER * 8, 256), BF16),
            pltpu.VMEM((GROUPS, PER * 8, 512), BF16),
            pltpu.VMEM((512, 1024), F32),
            pieces,
            pieces,
            pieces,
            pieces,
            pltpu.VMEM((4, 1, 128), F32),
            pltpu.VMEM((32, 1, 128), F32),
            pltpu.VMEM((4, 128, 512), BF16),
            pltpu.VMEM((4, 128, 512), BF16),
        ]
        + [dma] * 7
        + [dma((3,))]
        + slot_buffers(),
        compiler_params=pltpu.CompilerParams(
            collective_id=0, has_side_effects=True, vmem_limit_bytes=62 * 1024 * 1024
        ),
    )(
        resid, query, forget_logits, forget_margin.reshape(1, 512),
        jnp.pad(decay_spike.T, ((0, 4), (0, 0))), value_logits, output_gate_logits,
        head_norm_scale.reshape(1, 512), output_matrix, norm_scale_vector.reshape(1, 2048),
        routes.T, routing_weight.T, gate, up, down,
    )


def solution(mesh):
    whole = ("sp", "tp")
    rows, heads, experts = P(whole, None), P("sp", "tp"), P(whole, None, None)
    return jax.shard_map(
        layer,
        mesh=mesh,
        in_specs=(
            rows, heads, heads, P("tp"), heads, heads, heads, P("tp"), P(), P(), rows, rows,
            experts, experts, experts,
        ),
        out_specs=rows,
        check_vma=False,
    )
```

```python
import jax
import jax.numpy as jnp
from jax import lax
from jax.experimental import pallas as pl
from jax.experimental.pallas import tpu as pltpu
from jax.sharding import PartitionSpec as P

MESH = pl.DeviceIdType.MESH
F32 = jnp.float32
BF16 = jnp.bfloat16
I32 = jnp.int32
GROUPS = 4
PER = 32


def coords():
    sp = lax.axis_index("sp")
    return sp // 8, (sp // 2) % 4, sp % 2, lax.axis_index("tp")


def wrap(value, size):
    return jnp.where(value >= size, value - size, value)


def entry_barrier():
    barrier = pltpu.get_barrier_semaphore()
    sp, x = lax.axis_index("sp"), lax.axis_index("tp")
    others = [wrap(x + k, 4) for k in range(1, 4)]
    for other in others:
        pl.semaphore_signal(barrier, inc=1, device_id=(sp, other), device_id_type=MESH)

    @pl.loop(1, 32)
    def _(p):
        for other in [x] + others:
            pl.semaphore_signal(
                barrier, inc=1, device_id=(wrap(sp + p, 32), other), device_id_type=MESH
            )

    return barrier


def iota(shape, dim):
    return lax.broadcasted_iota(I32, shape, dim)


def slot_tables(routes, weights, pack_l, comb_l):
    z, y, c, x = coords()
    d = iota((128, 128), 0)
    dz, dy, dc = (d >> 3) & 3, (d >> 1) & 3, d & 1
    dx = ((d >> 5) + 8 - dz - dy) & 3
    expert = (((((z + dz) & 3) * 4 + ((y + dy) & 3)) * 2 + ((c + dc) & 1)) * 4) + ((x + dx) & 3)
    first = routes[0:1, :] == expert
    second = routes[1:2, :] == expert
    member = jnp.where(first, 1.0, jnp.where(second, 1.0, 0.0))
    earlier = jnp.where(iota((128, 128), 0) < iota((128, 128), 1), 1.0, 0.0).astype(BF16)
    rank = jnp.dot(member.astype(BF16), earlier, preferred_element_type=F32)
    code = (member * (rank + 1.0)).astype(BF16)
    share = jnp.where(first, weights[0:1, :], jnp.where(second, weights[1:2, :], 0.0))
    high = share.astype(BF16)
    low = (share - high.astype(F32)).astype(BF16)
    table = jnp.concatenate([code, high, low], axis=1)
    rows = PER * 8
    at = iota((rows, 128), 0)
    wanted = ((at & 3) + 1).astype(F32)
    upper = ((at >> 2) & 1) == 0
    for g in range(GROUPS):
        spread = jnp.where((at >> 3) + g * PER == iota((rows, 128), 1), 1.0, 0.0).astype(BF16)
        wide = jnp.dot(spread, table, preferred_element_type=F32)
        chosen = wide[:, :128] == wanted
        one = jnp.where(chosen, 1.0, 0.0)
        high_g = jnp.where(chosen, wide[:, 128:256], 0.0)
        low_g = jnp.where(chosen, wide[:, 256:], 0.0)
        zero = jnp.zeros_like(one)
        pack_l[g] = jnp.concatenate(
            [jnp.where(upper, one, zero), jnp.where(upper, zero, one)], axis=1
        ).astype(BF16)
        comb_l[g] = jnp.concatenate(
            [
                jnp.where(upper, high_g, zero),
                jnp.where(upper, zero, high_g),
                jnp.where(upper, low_g, zero),
                jnp.where(upper, zero, low_g),
            ],
            axis=1,
        ).astype(BF16)


def blocks(ref, lo, count):
    return ref.at[pl.ds(lo, count)]


def wait_group(buf, sem, g):
    z, y, c, x = coords()
    other = (lax.axis_index("sp"), (x + 1) % 4)

    @pl.when(g == 0)
    def _():
        part = blocks(buf, 1, PER - 1)
        pltpu.make_async_remote_copy(part, part, sem, sem, other, MESH).wait_recv()

    @pl.when(g > 0)
    def _():
        part = blocks(buf, g * PER, PER)
        pltpu.make_async_remote_copy(part, part, sem, sem, other, MESH).wait_recv()


def send_group(src, dst, send_sem, recv_sem, g, sign):
    z, y, c, x = coords()
    turned = g if sign > 0 else 4 - g
    rows = [2 * wrap(y + (dy if sign > 0 else (4 - dy) % 4), 4) for dy in range(4)]
    cores = [c, 1 - c]

    def one(dz):
        plane = 8 * wrap(z + dz if sign > 0 else z + 4 - dz, 4)
        start = x + turned + (4 - dz if sign > 0 else dz)
        for dy in range(4):
            column = (start + (4 - dy if sign > 0 else dy)) % 4
            for dc in range(2):
                d = g * PER + dz * 8 + dy * 2 + dc
                copy = pltpu.make_async_remote_copy(
                    src.at[d], dst.at[d], send_sem, recv_sem,
                    (plane + rows[dy] + cores[dc], column), MESH,
                )
                if dy == 0 and dc == 0:
                    pl.when(d > 0)(copy.start)
                else:
                    copy.start()

    pl.loop(0, 4)(one)


def wait_sent(buf, sem):
    x = lax.axis_index("tp")
    part = blocks(buf, 1, GROUPS * PER - 1)
    pltpu.make_async_remote_copy(
        part, part, sem, sem, (lax.axis_index("sp"), (x + 1) % 4), MESH
    ).wait_send()


def expert_phase(stream, normed, pack_l, comb_l, gate, up, down, weight_copies, bufs, total, out):
    out_slots, in_slots, answers, replies, send_sem, recv_sem, send_back, recv_back = bufs
    halves = jnp.concatenate([normed[:, :1024], normed[:, 1024:]], axis=0)
    for g in range(GROUPS):
        with jax.named_scope("pack"):
            packed = jnp.dot(pack_l[g], halves, preferred_element_type=F32).astype(BF16)
            out_slots[pl.ds(g * PER, PER)] = packed.reshape(PER, 8, 1024)
        with jax.named_scope("dispatch"):
            send_group(out_slots, in_slots, send_sem, recv_sem.at[g], g, 1)
    in_slots[0] = out_slots[0]
    for copy in weight_copies:
        copy.wait()
    rows = PER * 8
    a, b = iota((rows, rows), 0), iota((rows, rows), 1)
    place = ((a & 127) >> 2) * 8 + (a >> 7) * 4 + (a & 3)
    unpack = jnp.where(place == b, 1.0, 0.0).astype(BF16)
    place_b = ((b & 127) >> 2) * 8 + (b >> 7) * 4 + (b & 3)
    repack = jnp.where(place_b == a, 1.0, 0.0).astype(BF16)

    @pl.loop(0, GROUPS)
    def _(g):
        with jax.named_scope("slots_wait"):
            wait_group(in_slots, recv_sem.at[g], g)
        came = in_slots[pl.ds(g * PER, PER)].reshape(rows, 1024)
        flat = jnp.dot(unpack, came, preferred_element_type=F32).astype(BF16)
        x = jnp.concatenate([flat[:128], flat[128:]], axis=1)
        hidden = []
        for n in range(0, 1024, 256):
            gated = jnp.dot(x, gate[:, n : n + 256], preferred_element_type=F32)
            lifted = jnp.dot(x, up[:, n : n + 256], preferred_element_type=F32)
            hidden.append((gated * jax.nn.sigmoid(gated) * lifted).astype(BF16))
        hidden = jnp.concatenate(hidden, axis=1)
        y0 = jnp.dot(hidden, down[:, :1024], preferred_element_type=F32).astype(BF16)
        y1 = jnp.dot(hidden, down[:, 1024:], preferred_element_type=F32).astype(BF16)
        both = jnp.concatenate([y0, y1], axis=0)
        back = jnp.dot(repack, both, preferred_element_type=F32).astype(BF16)
        answers[pl.ds(g * PER, PER)] = back.reshape(PER, 8, 1024)
        with jax.named_scope("answer_send"):
            send_group(answers, replies, send_back, recv_back.at[g], g, -1)

    replies[0] = answers[0]
    total[...] = jnp.zeros_like(total)

    @pl.loop(0, GROUPS)
    def _(g):
        with jax.named_scope("replies_wait"):
            wait_group(replies, recv_back.at[g], g)
        got = replies[pl.ds(g * PER, PER)].reshape(rows, 1024)
        total[...] += lax.dot_general(
            comb_l[g], got, (((0,), (0,)), ((), ())), preferred_element_type=F32
        )

    for h in range(2):
        part = total[h * 128 : h * 128 + 128] + total[256 + h * 128 : 256 + h * 128 + 128]
        cols = slice(h * 1024, h * 1024 + 1024)
        out[:, cols] = (stream[:, cols].astype(F32) + part).astype(BF16)
    wait_sent(out_slots, send_sem)
    wait_sent(answers, send_back)


def slot_buffers():
    slots = pltpu.VMEM((GROUPS * PER, 8, 1024), BF16)
    dma = pltpu.SemaphoreType.DMA
    return [slots] * 4 + [dma, dma((GROUPS,)), dma, dma((GROUPS,))]


def sp_peer(i):
    return (i, lax.axis_index("tp"))


def tp_peer(i):
    return (lax.axis_index("sp"), i)


def dot_nt(a, b):
    return lax.dot_general(a, b, (((1,), (1,)), ((), ())), preferred_element_type=F32)


def dot_tn(a, b):
    return lax.dot_general(a, b, (((0,), (0,)), ((), ())), preferred_element_type=F32)


def dot(a, b):
    return jnp.dot(a, b, preferred_element_type=F32)


def split(value):
    high = value.astype(BF16)
    return high, (value - high.astype(F32)).astype(BF16)


def spike_sums(spikes, run_row, run_col):
    at_or_before = jnp.where(iota((512, 512), 0) <= iota((512, 512), 1), 1.0, 0.0).astype(BF16)
    after = jnp.where(iota((512, 512), 0) >= iota((512, 512), 1), 1.0, 0.0).astype(BF16)
    rest = jnp.concatenate([spikes[...], jnp.zeros((4, 512), F32)], axis=0)
    row, col = jnp.zeros((8, 512), F32), jnp.zeros((512, 8), F32)
    for _ in range(3):
        part = rest.astype(BF16)
        rest = rest - part.astype(F32)
        row = row + dot(part, at_or_before)
        col = col + dot_nt(after, part)
    run_row[...] = row
    run_col[...] = col


def channel_pass(query, forget, value, margin, qd, kd, vv, last):
    lower = jnp.where(iota((128, 128), 0) >= iota((128, 128), 1), 1.0, 0.0).astype(BF16)
    last[...] = jnp.zeros_like(last)

    @pl.loop(0, 4)
    def _(b):
        rows = pl.ds(pl.multiple_of(b * 128, 128), 128)
        for n in range(0, 512, 128):
            cols = slice(n, n + 128)
            keys = margin[:, cols] * jax.nn.sigmoid(-forget[rows, cols].astype(F32))
            high, low = split(jnp.log1p(-keys))
            run = dot(lower, high) + dot(lower, low) + last[:, cols]
            last[:, cols] = run[127:128]
            kd[rows, cols] = (keys * jnp.exp(-run)).astype(BF16)
            qd[rows, cols] = (query[rows, cols].astype(F32) * jnp.exp(run) * 128**-0.5).astype(BF16)
            logits = value[rows, cols].astype(F32)
            vv[rows, cols] = (logits * jax.nn.sigmoid(logits)).astype(BF16)


def own_states(kd, vv, last, run_row, run_col, state_out, decay_out):
    for h in range(4):
        cols = slice(h * 128, h * 128 + 128)
        total = run_row[h : h + 1, 511:512]
        fade = jnp.exp(total - run_col[:, h : h + 1])
        keys = (kd[:, cols].astype(F32) * fade).astype(BF16)
        state = dot_tn(vv[:, cols], keys) * jnp.exp(last[:, cols])
        state_out[pl.ds(h * 8, 8)] = state.astype(BF16).reshape(8, 16, 128)
        decay_out[h] = last[:, cols] + total


def within_pass(qd, kd, vv, run_row, run_col, local):
    causal = iota((128, 128), 0) >= iota((128, 128), 1)
    for h in range(4):
        cols = slice(h * 128, h * 128 + 128)
        for i in range(4):
            rows = slice(i * 128, i * 128 + 128)
            seen = (i + 1) * 128
            scores = dot_nt(qd[rows, cols], kd[:seen, cols])
            gap = run_col[rows, h : h + 1] - run_row[h : h + 1, :seen]
            edge = slice(i * 128, seen)
            inner = jnp.where(causal, scores[:, edge] * jnp.exp(jnp.where(causal, gap[:, edge], 0.0)), 0.0)
            parts = [inner.astype(BF16)]
            if i:
                parts.insert(0, (scores[:, : i * 128] * jnp.exp(gap[:, : i * 128])).astype(BF16))
            weights = jnp.concatenate(parts, axis=1)
            local[rows, cols] = dot(weights, vv[:seen, cols])


def send_states(state_out, decay_out, state_in, decay_in, sems):
    me = lax.axis_index("sp")
    send, recv, send_d, recv_d = sems

    @pl.loop(1, 32)
    def _(d):
        p = wrap(me + d, 32)
        pltpu.make_async_remote_copy(
            decay_out.at[p // 8], decay_in.at[me], send_d, recv_d, sp_peer(p), MESH
        ).start()
        pltpu.make_async_remote_copy(
            state_out.at[p], state_in.at[me], send, recv, sp_peer(p), MESH
        ).start()

    state_in[me] = state_out[me]
    decay_in[me] = decay_out[me // 8]


def wait_bytes(part, sem, sent):
    copy = pltpu.make_async_remote_copy(
        part, part, sem, sem, tp_peer((lax.axis_index("tp") + 1) % 4), MESH
    )
    if sent:
        copy.wait_send()
    else:
        copy.wait_recv()


def scan_states(state_in, decay_in, prior_out, prior_in, sems, back):
    send, recv, send_d, recv_d = sems
    wait_bytes(state_in.at[pl.ds(0, 31)], recv, False)
    wait_bytes(decay_in.at[pl.ds(0, 31)], recv_d, False)
    state = jnp.zeros((16, 128), F32)
    for i in range(32):
        prior_out[i] = state.astype(BF16)
        state = jnp.exp(decay_in[i]) * state + state_in[i].astype(F32)
    me = lax.axis_index("sp")

    @pl.loop(1, 32)
    def _(d):
        p = wrap(me + d, 32)
        pltpu.make_async_remote_copy(
            prior_out.at[p], prior_in.at[me], back[0], back[1], sp_peer(p), MESH
        ).start()

    prior_in[me] = prior_out[me]


def gate_factors(qd, run_col, out_gate, head_scale, factor):
    @pl.loop(0, 4)
    def _(b):
        rows = pl.ds(pl.multiple_of(b * 128, 128), 128)
        for h in range(4):
            cols = slice(h * 128, h * 128 + 128)
            logits = out_gate[rows, cols].astype(F32)
            factor[rows, cols] = head_scale[:, cols] * (logits * jax.nn.sigmoid(logits))
            qd[rows, cols] = (
                qd[rows, cols].astype(F32) * jnp.exp(run_col[rows, h : h + 1])
            ).astype(BF16)


def gate_pass(asked, local, prior_in, factor, gated_out, gated_in, sems):
    x = lax.axis_index("tp")
    for k, ahead in enumerate((2, 1, 3, 0)):
        j = wrap(x + ahead, 4)
        rows = pl.ds(pl.multiple_of(j * 128, 128), 128)
        for h in range(4):
            cols = slice(h * 128, h * 128 + 128)
            prior = prior_in[pl.ds(h * 8, 8)].reshape(128, 128)
            full = local[rows, cols] + dot_nt(asked[rows, cols], prior)
            square = jnp.mean(full * full, axis=1, keepdims=True)
            gated_out[j, :, cols] = (full * lax.rsqrt(square + 1e-06) * factor[rows, cols]).astype(BF16)
        if ahead:
            pltpu.make_async_remote_copy(
                gated_out.at[j], gated_in.at[x], sems[0], sems[1].at[k], tp_peer(j), MESH
            ).start()
        else:
            gated_in[x] = gated_out[x]


def project(gated_in, matrix, mixed, sems):
    x = lax.axis_index("tp")
    mixed[...] = dot(gated_in[x], matrix[pl.ds(pl.multiple_of(x * 512, 512), 512)])
    for k, back in ((1, 3), (2, 1), (0, 2)):
        i = wrap(x + back, 4)
        wait_bytes(gated_in.at[i], sems[1].at[k], False)
        mixed[...] += dot(gated_in[i], matrix[pl.ds(pl.multiple_of(i * 512, 512), 512)])


def layer_kernel(
    resid_hbm, query_hbm, forget_hbm, margin, spikes, value_hbm, gate_logits_hbm, head_scale,
    matrix_hbm, scale, routes, weights, gate_hbm, up_hbm, down_hbm, out,
    resid, query, forget, value, gate_logits, matrix, gate, up, down, in_sems,
    qd, kd, vv, last, run_row, run_col, local, factor, mixed, pack_l, comb_l, total,
    state_out, state_in, prior_out, prior_in, decay_out, decay_in, gated_out, gated_in,
    state_send, state_recv, decay_send, decay_recv, prior_send, prior_recv, gated_send, gated_recv,
    *bufs,
):
    moves = [
        (forget_hbm, forget), (query_hbm, query), (value_hbm, value), (gate_logits_hbm, gate_logits),
        (resid_hbm, resid), (matrix_hbm, matrix), (gate_hbm.at[0], gate), (up_hbm.at[0], up),
        (down_hbm.at[0], down),
    ]
    copies = [pltpu.make_async_copy(src, dst, in_sems.at[i]) for i, (src, dst) in enumerate(moves)]
    for copy in copies:
        copy.start()
    with jax.named_scope("greet"):
        barrier = entry_barrier()
    with jax.named_scope("spikes"):
        spike_sums(spikes, run_row, run_col)
    with jax.named_scope("inputs"):
        for copy in copies[:3]:
            copy.wait()
    with jax.named_scope("channels"):
        channel_pass(query, forget, value, margin, qd, kd, vv, last)
    with jax.named_scope("states"):
        own_states(kd, vv, last, run_row, run_col, state_out, decay_out)
    with jax.named_scope("met"):
        pl.semaphore_wait(barrier, GROUPS * PER - 1)
    sems = (state_send, state_recv, decay_send, decay_recv)
    with jax.named_scope("state_send"):
        send_states(state_out, decay_out, state_in, decay_in, sems)
    with jax.named_scope("within"):
        within_pass(qd, kd, vv, run_row, run_col, local)
    with jax.named_scope("tables"):
        slot_tables(routes, weights, pack_l, comb_l)
    with jax.named_scope("factors"):
        copies[3].wait()
        gate_factors(qd, run_col, gate_logits, head_scale, factor)
    back = (prior_send, prior_recv)
    with jax.named_scope("scan"):
        scan_states(state_in, decay_in, prior_out, prior_in, sems, back)
    with jax.named_scope("prior_wait"):
        wait_bytes(prior_in.at[pl.ds(0, 31)], prior_recv, False)
    gated = (gated_send, gated_recv)
    with jax.named_scope("gating"):
        gate_pass(qd, local, prior_in, factor, gated_out, gated_in, gated)
    copies[4].wait()
    copies[5].wait()
    with jax.named_scope("project"):
        project(gated_in, matrix, mixed, gated)
    stream = (resid[...].astype(F32) + mixed[...]).astype(BF16)
    resid[...] = stream
    values = stream.astype(F32)
    square = jnp.mean(values * values, axis=1, keepdims=True)
    normed = (values * lax.rsqrt(square + 1e-06) * scale[...]).astype(BF16)
    with jax.named_scope("experts"):
        expert_phase(resid, normed, pack_l, comb_l, gate, up, down, copies[6:], bufs, total, out)
    wait_bytes(state_out.at[pl.ds(0, 31)], state_send, True)
    wait_bytes(decay_in.at[pl.ds(0, 31)], decay_send, True)
    wait_bytes(prior_out.at[pl.ds(0, 31)], prior_send, True)
    wait_bytes(gated_out.at[pl.ds(0, 3)], gated_send, True)


def layer(
    resid, query, forget_logits, forget_margin, decay_spike, value_logits, output_gate_logits,
    head_norm_scale, output_matrix, norm_scale_vector, routes, routing_weight, gate, up, down,
):
    vmem = pl.BlockSpec(memory_space=pltpu.VMEM)
    hbm = pl.BlockSpec(memory_space=pl.ANY)
    dma = pltpu.SemaphoreType.DMA
    wide = pltpu.VMEM((512, 512), BF16)
    pieces = pltpu.VMEM((32, 16, 128), BF16)
    return pl.pallas_call(
        layer_kernel,
        out_shape=pltpu.VMEM((128, 2048), BF16),
        in_specs=[hbm, hbm, hbm, vmem, vmem, hbm, hbm, vmem, hbm, vmem, vmem, vmem, hbm, hbm, hbm],
        out_specs=vmem,
        scratch_shapes=[
            pltpu.VMEM((128, 2048), BF16),
            wide,
            wide,
            wide,
            wide,
            pltpu.VMEM((2048, 2048), BF16),
            pltpu.VMEM((2048, 1024), BF16),
            pltpu.VMEM((2048, 1024), BF16),
            pltpu.VMEM((1024, 2048), BF16),
            dma((9,)),
            wide,
            wide,
            wide,
            pltpu.VMEM((1, 512), F32),
            pltpu.VMEM((8, 512), F32),
            pltpu.VMEM((512, 8), F32),
            pltpu.VMEM((512, 512), F32),
            pltpu.VMEM((512, 512), F32),
            pltpu.VMEM((128, 2048), F32),
            pltpu.VMEM((GROUPS, PER * 8, 256), BF16),
            pltpu.VMEM((GROUPS, PER * 8, 512), BF16),
            pltpu.VMEM((512, 1024), F32),
            pieces,
            pieces,
            pieces,
            pieces,
            pltpu.VMEM((4, 1, 128), F32),
            pltpu.VMEM((32, 1, 128), F32),
            pltpu.VMEM((4, 128, 512), BF16),
            pltpu.VMEM((4, 128, 512), BF16),
        ]
        + [dma] * 7
        + [dma((3,))]
        + slot_buffers(),
        compiler_params=pltpu.CompilerParams(
            collective_id=0, has_side_effects=True, vmem_limit_bytes=62 * 1024 * 1024
        ),
    )(
        resid, query, forget_logits, forget_margin.reshape(1, 512),
        decay_spike.T, value_logits, output_gate_logits,
        head_norm_scale.reshape(1, 512), output_matrix, norm_scale_vector.reshape(1, 2048),
        routes.T, routing_weight.T, gate, up, down,
    )


def solution(mesh):
    whole = ("sp", "tp")
    rows, heads, experts = P(whole, None), P("sp", "tp"), P(whole, None, None)
    return jax.shard_map(
        layer,
        mesh=mesh,
        in_specs=(
            rows, heads, heads, P("tp"), heads, heads, heads, P("tp"), P(), P(), rows, rows,
            experts, experts, experts,
        ),
        out_specs=rows,
        check_vma=False,
    )
```

```python
import jax
import jax.numpy as jnp
from jax import lax
from jax.experimental import pallas as pl
from jax.experimental.pallas import tpu as pltpu
from jax.sharding import PartitionSpec as P

MESH = pl.DeviceIdType.MESH
F32 = jnp.float32
BF16 = jnp.bfloat16
I32 = jnp.int32
GROUPS = 4
PER = 32


def coords():
    sp = lax.axis_index("sp")
    return sp // 8, (sp // 2) % 4, sp % 2, lax.axis_index("tp")


def wrap(value, size):
    return jnp.where(value >= size, value - size, value)


def entry_barrier():
    barrier = pltpu.get_barrier_semaphore()
    sp, x = lax.axis_index("sp"), lax.axis_index("tp")

    for low, top in ((16, 32), (1, 16)):

        @pl.loop(low, top)
        def _(p):
            pl.semaphore_signal(barrier, inc=1, device_id=(wrap(sp + p, 32), x), device_id_type=MESH)

    for k in range(1, 4):
        pl.semaphore_signal(barrier, inc=1, device_id=(sp, wrap(x + k, 4)), device_id_type=MESH)
    return barrier


def iota(shape, dim):
    return lax.broadcasted_iota(I32, shape, dim)


def slot_tables(routes, weights, pack_l, comb_l):
    z, y, c, x = coords()
    d = iota((128, 128), 0)
    dz, dy, dc = (d >> 3) & 3, (d >> 1) & 3, d & 1
    dx = ((d >> 5) + 8 - dz - dy) & 3
    expert = (((((z + dz) & 3) * 4 + ((y + dy) & 3)) * 2 + ((c + dc) & 1)) * 4) + ((x + dx) & 3)
    first = routes[0:1, :] == expert
    second = routes[1:2, :] == expert
    member = jnp.where(first, 1.0, jnp.where(second, 1.0, 0.0))
    earlier = jnp.where(iota((128, 128), 0) < iota((128, 128), 1), 1.0, 0.0).astype(BF16)
    rank = jnp.dot(member.astype(BF16), earlier, preferred_element_type=F32)
    code = (member * (rank + 1.0)).astype(BF16)
    share = jnp.where(first, weights[0:1, :], jnp.where(second, weights[1:2, :], 0.0))
    table = jnp.concatenate([code, share.astype(BF16)], axis=1)
    rows = PER * 8
    at = iota((rows, 128), 0)
    wanted = ((at & 3) + 1).astype(F32)
    upper = ((at >> 2) & 1) == 0
    for g in range(GROUPS):
        spread = jnp.where((at >> 3) + g * PER == iota((rows, 128), 1), 1.0, 0.0).astype(BF16)
        wide = jnp.dot(spread, table, preferred_element_type=F32)
        chosen = wide[:, :128] == wanted
        one = jnp.where(chosen, 1.0, 0.0)
        weighed = jnp.where(chosen, wide[:, 128:], 0.0)
        zero = jnp.zeros_like(one)
        pack_l[g] = jnp.concatenate(
            [jnp.where(upper, one, zero), jnp.where(upper, zero, one)], axis=1
        ).astype(BF16)
        comb_l[g] = jnp.concatenate(
            [jnp.where(upper, weighed, zero), jnp.where(upper, zero, weighed)], axis=1
        ).astype(BF16)


def blocks(ref, lo, count):
    return ref.at[pl.ds(lo, count)]


def wait_group(buf, sem, g):
    z, y, c, x = coords()
    other = (lax.axis_index("sp"), (x + 1) % 4)

    @pl.when(g == 0)
    def _():
        part = blocks(buf, 1, PER - 1)
        pltpu.make_async_remote_copy(part, part, sem, sem, other, MESH).wait_recv()

    @pl.when(g > 0)
    def _():
        part = blocks(buf, g * PER, PER)
        pltpu.make_async_remote_copy(part, part, sem, sem, other, MESH).wait_recv()


def send_group(src, dst, send_sem, recv_sem, g, sign):
    z, y, c, x = coords()
    turned = g if sign > 0 else 4 - g
    rows = [2 * wrap(y + (dy if sign > 0 else (4 - dy) % 4), 4) for dy in range(4)]
    cores = [c, 1 - c]

    def one(dz):
        plane = 8 * wrap(z + dz if sign > 0 else z + 4 - dz, 4)
        start = x + turned + (4 - dz if sign > 0 else dz)
        for dy in range(4):
            column = (start + (4 - dy if sign > 0 else dy)) % 4
            for dc in range(2):
                d = g * PER + dz * 8 + dy * 2 + dc
                copy = pltpu.make_async_remote_copy(
                    src.at[d], dst.at[d], send_sem, recv_sem,
                    (plane + rows[dy] + cores[dc], column), MESH,
                )
                if dy == 0 and dc == 0:
                    pl.when(d > 0)(copy.start)
                else:
                    copy.start()

    pl.loop(0, 4)(one)


def wait_sent(buf, sem):
    x = lax.axis_index("tp")
    part = blocks(buf, 1, GROUPS * PER - 1)
    pltpu.make_async_remote_copy(
        part, part, sem, sem, (lax.axis_index("sp"), (x + 1) % 4), MESH
    ).wait_send()


def expert_phase(stream, normed, pack_l, comb_l, gate, up, down, weight_copies, bufs, total, out):
    out_slots, in_slots, answers, replies, send_sem, recv_sem, send_back, recv_back = bufs
    halves = jnp.concatenate([normed[:, :1024], normed[:, 1024:]], axis=0)
    for g in range(GROUPS):
        with jax.named_scope("pack"):
            packed = jnp.dot(pack_l[g], halves, preferred_element_type=F32).astype(BF16)
            out_slots[pl.ds(g * PER, PER)] = packed.reshape(PER, 8, 1024)
        with jax.named_scope("dispatch"):
            send_group(out_slots, in_slots, send_sem, recv_sem.at[g], g, 1)
    in_slots[0] = out_slots[0]
    for copy in weight_copies:
        copy.wait()
    rows = PER * 8
    a, b = iota((rows, rows), 0), iota((rows, rows), 1)
    place = ((a & 127) >> 2) * 8 + (a >> 7) * 4 + (a & 3)
    unpack = jnp.where(place == b, 1.0, 0.0).astype(BF16)
    place_b = ((b & 127) >> 2) * 8 + (b >> 7) * 4 + (b & 3)
    repack = jnp.where(place_b == a, 1.0, 0.0).astype(BF16)

    @pl.loop(0, GROUPS)
    def _(g):
        with jax.named_scope("slots_wait"):
            wait_group(in_slots, recv_sem.at[g], g)
        came = in_slots[pl.ds(g * PER, PER)].reshape(rows, 1024)
        flat = jnp.dot(unpack, came, preferred_element_type=F32).astype(BF16)
        x = jnp.concatenate([flat[:128], flat[128:]], axis=1)
        hidden = []
        for n in range(0, 1024, 256):
            gated = jnp.dot(x, gate[:, n : n + 256], preferred_element_type=F32)
            lifted = jnp.dot(x, up[:, n : n + 256], preferred_element_type=F32)
            hidden.append((gated * logistic(gated) * lifted).astype(BF16))
        hidden = jnp.concatenate(hidden, axis=1)
        y0 = jnp.dot(hidden, down[:, :1024], preferred_element_type=F32).astype(BF16)
        y1 = jnp.dot(hidden, down[:, 1024:], preferred_element_type=F32).astype(BF16)
        both = jnp.concatenate([y0, y1], axis=0)
        back = jnp.dot(repack, both, preferred_element_type=F32).astype(BF16)
        answers[pl.ds(g * PER, PER)] = back.reshape(PER, 8, 1024)
        with jax.named_scope("answer_send"):
            send_group(answers, replies, send_back, recv_back.at[g], g, -1)

    replies[0] = answers[0]
    total[...] = jnp.zeros_like(total)

    def gathered(g):
        with jax.named_scope("replies_wait"):
            wait_group(replies, recv_back.at[g], g)
        return dot_tn(comb_l[g], replies[pl.ds(g * PER, PER)].reshape(rows, 1024))

    @pl.loop(0, GROUPS - 1)
    def _(g):
        total[...] += gathered(g)

    summed = total[...] + gathered(GROUPS - 1)
    for h in range(2):
        cols = slice(h * 1024, h * 1024 + 1024)
        out[:, cols] = (stream[:, cols].astype(F32) + summed[h * 128 : h * 128 + 128]).astype(BF16)
    wait_sent(out_slots, send_sem)
    wait_sent(answers, send_back)


def slot_buffers():
    slots = pltpu.VMEM((GROUPS * PER, 8, 1024), BF16)
    dma = pltpu.SemaphoreType.DMA
    return [slots] * 4 + [dma, dma((GROUPS,)), dma, dma((GROUPS,))]


def sp_peer(i):
    return (i, lax.axis_index("tp"))


def tp_peer(i):
    return (lax.axis_index("sp"), i)


def dot_nt(a, b):
    return lax.dot_general(a, b, (((1,), (1,)), ((), ())), preferred_element_type=F32)


def dot_tn(a, b):
    return lax.dot_general(a, b, (((0,), (0,)), ((), ())), preferred_element_type=F32)


def dot(a, b):
    return jnp.dot(a, b, preferred_element_type=F32)


def split(value):
    high = value.astype(BF16)
    return high, (value - high.astype(F32)).astype(BF16)


def logistic(value):
    return 0.5 * jnp.tanh(0.5 * value) + 0.5


def fill_triangle(tri):
    tri[...] = jnp.where(iota((256, 256), 0) >= iota((256, 256), 1), 1.0, 0.0).astype(BF16)


def spike_sums(spikes, tri, run_row, run_col):
    high, low = split(jnp.concatenate([spikes[...], jnp.zeros((4, 512), F32)], axis=0))
    parts = jnp.concatenate([high[:, :256], low[:, :256], high[:, 256:], low[:, 256:]], axis=0)
    sums = dot_nt(parts, tri[...])
    early = sums[:8] + sums[8:16]
    row = jnp.concatenate([early, sums[16:24] + sums[24:] + early[:, 255:256]], axis=1)
    run_row[...] = row
    run_col[...] = row.T


def key_head(h, forget, value, margin, tri, run_row, fade, runs, kd, vv, state_out, decay_out):
    cols = slice(h * 128, h * 128 + 128)
    keys = margin[:, cols] * logistic(-forget[:, cols].astype(F32))
    logs = jnp.concatenate(split(jnp.log1p(-keys)), axis=1)
    early, late = dot(tri[...], logs[:256]), dot(tri[...], logs[256:])
    early = early[:, :128] + early[:, 128:]
    run = jnp.concatenate([early, late[:, :128] + late[:, 128:] + early[255:]], axis=0)
    runs[:, cols] = run
    raised = keys * jnp.exp(-run)
    kd[:, cols] = raised.astype(BF16)
    logits = value[:, cols].astype(F32)
    values = (logits * logistic(logits)).astype(BF16)
    vv[:, cols] = values
    last = run[511:512]
    state = dot_tn(values, (raised * fade[:, h : h + 1]).astype(BF16)) * jnp.exp(last)
    state_out[pl.ds(h * 8, 8)] = state.astype(BF16).reshape(8, 16, 128)
    decay_out[h] = last + run_row[h : h + 1, 511:512]


def query_pass(query, runs, run_col, qd, asked):
    grow = jnp.exp(run_col[...])
    for h in range(4):
        cols = slice(h * 128, h * 128 + 128)
        faded = query[:, cols].astype(F32) * (jnp.exp(runs[:, cols]) * 128**-0.5)
        twice = slice(h * 256, h * 256 + 256)
        qd[:, twice] = jnp.concatenate(split(faded), axis=1)
        asked[:, twice] = jnp.concatenate(split(faded * grow[:, h : h + 1]), axis=1)


def within_pass(qd, kd, vv, run_row, run_col, local):
    causal = iota((128, 128), 0) >= iota((128, 128), 1)
    for h in range(4):
        cols = slice(h * 128, h * 128 + 128)
        for i in range(4):
            rows = slice(i * 128, i * 128 + 128)
            seen = (i + 1) * 128
            keys = kd[:seen, cols]
            scores = dot_nt(
                qd[rows, h * 256 : h * 256 + 256], jnp.concatenate([keys, keys], axis=1)
            )
            gap = run_col[rows, h : h + 1] - run_row[h : h + 1, :seen]
            edge = slice(i * 128, seen)
            inner = jnp.where(causal, scores[:, edge] * jnp.exp(jnp.where(causal, gap[:, edge], 0.0)), 0.0)
            parts = [inner.astype(BF16)]
            if i:
                parts.insert(0, (scores[:, : i * 128] * jnp.exp(gap[:, : i * 128])).astype(BF16))
            weights = jnp.concatenate(parts, axis=1)
            local[rows, cols] = dot(weights, vv[:seen, cols])


def send_states(state_out, decay_out, state_in, decay_in, sems):
    me = lax.axis_index("sp")
    send, recv, send_d, recv_d = sems
    for low, top in ((16, 32), (1, 16)):

        @pl.loop(low, top)
        def _(d):
            p = wrap(me + d, 32)
            pltpu.make_async_remote_copy(
                state_out.at[p], state_in.at[me], send, recv, sp_peer(p), MESH
            ).start()
            pltpu.make_async_remote_copy(
                decay_out.at[p // 8], decay_in.at[me], send_d, recv_d, sp_peer(p), MESH
            ).start()

    state_in[me] = state_out[me]
    decay_in[me] = decay_out[me // 8]


def wait_bytes(part, sem, sent):
    copy = pltpu.make_async_remote_copy(
        part, part, sem, sem, tp_peer((lax.axis_index("tp") + 1) % 4), MESH
    )
    if sent:
        copy.wait_send()
    else:
        copy.wait_recv()


def scan_states(state_in, decay_in, prior_out, prior_in, sems, back):
    send, recv, send_d, recv_d = sems
    wait_bytes(state_in.at[pl.ds(0, 31)], recv, False)
    wait_bytes(decay_in.at[pl.ds(0, 31)], recv_d, False)
    state = jnp.zeros((16, 128), F32)
    for i in range(32):
        prior_out[i] = state.astype(BF16)
        state = jnp.exp(decay_in[i]) * state + state_in[i].astype(F32)
    me = lax.axis_index("sp")

    for low, top in ((16, 32), (1, 16)):

        @pl.loop(low, top)
        def _(d):
            p = wrap(me + d, 32)
            pltpu.make_async_remote_copy(
                prior_out.at[p], prior_in.at[me], back[0], back[1], sp_peer(p), MESH
            ).start()

    prior_in[me] = prior_out[me]


def gate_factors(out_gate, head_scale, factor):
    logits = out_gate[...].astype(F32)
    factor[...] = head_scale[...] * (logits * logistic(logits))


def gate_pass(asked, local, prior_in, factor, gated_out, gated_in, sems):
    x = lax.axis_index("tp")
    for k, ahead in enumerate((2, 1, 3, 0)):
        j = wrap(x + ahead, 4)
        rows = pl.ds(pl.multiple_of(j * 128, 128), 128)
        for h in range(4):
            cols = slice(h * 128, h * 128 + 128)
            prior = prior_in[pl.ds(h * 8, 8)].reshape(128, 128)
            ask = asked[rows, h * 256 : h * 256 + 256]
            full = local[rows, cols] + dot_nt(ask, jnp.concatenate([prior, prior], axis=1))
            square = jnp.mean(full * full, axis=1, keepdims=True)
            gated_out[j, :, cols] = (full * lax.rsqrt(square + 1e-06) * factor[rows, cols]).astype(BF16)
        if ahead:
            pltpu.make_async_remote_copy(
                gated_out.at[j], gated_in.at[x], sems[0], sems[1].at[k], tp_peer(j), MESH
            ).start()
        else:
            gated_in[x] = gated_out[x]


def project(gated_in, matrix, mixed, sems):
    x = lax.axis_index("tp")

    def product(i):
        return dot(gated_in[i], matrix[pl.ds(pl.multiple_of(i * 512, 512), 512)])

    mixed[...] = product(x)
    for k, back in ((0, 2), (1, 3), (2, 1)):
        i = wrap(x + back, 4)
        with jax.named_scope(f"tp_wait{k}"):
            wait_bytes(gated_in.at[i], sems[1].at[k], False)
        mixed[...] += product(i)


def layer_kernel(
    resid_hbm, query_hbm, forget_hbm, margin_hbm, spikes_hbm, value_hbm, gate_logits_hbm, head_scale_hbm,
    matrix_hbm, scale_hbm, routes_hbm, weights_hbm, gate_hbm, up_hbm, down_hbm, out,
    resid, query, forget, margin, spikes, value, gate_logits, head_scale, matrix, scale, routes,
    weights, gate, up, down, in_sems,
    tri, runs, qd, asked, kd, vv, run_row, run_col, local, factor, mixed, pack_l, comb_l, total,
    state_out, state_in, prior_out, prior_in, decay_out, decay_in, gated_out, gated_in,
    state_send, state_recv, decay_send, decay_recv, prior_send, prior_recv, gated_send, gated_recv,
    *bufs,
):
    moves = [
        (spikes_hbm, spikes), (margin_hbm, margin), (forget_hbm, forget), (value_hbm, value),
        (query_hbm, query), (routes_hbm, routes), (weights_hbm, weights), (gate_logits_hbm, gate_logits),
        (head_scale_hbm, head_scale), (resid_hbm, resid), (scale_hbm, scale), (matrix_hbm, matrix),
        (gate_hbm.at[0], gate), (up_hbm.at[0], up), (down_hbm.at[0], down),
    ]
    copies = [pltpu.make_async_copy(src, dst, in_sems.at[i]) for i, (src, dst) in enumerate(moves)]
    for copy in copies[:5]:
        copy.start()
    with jax.named_scope("greet"):
        barrier = entry_barrier()
    for copy in copies[5:]:
        copy.start()
    with jax.named_scope("triangle"):
        fill_triangle(tri)
    copies[0].wait()
    with jax.named_scope("spikes"):
        spike_sums(spikes, tri, run_row, run_col)
        fade = jnp.exp(run_col[511:512, :] - run_col[...])
    with jax.named_scope("inputs"):
        for copy in copies[1:4]:
            copy.wait()
    with jax.named_scope("keys"):
        for h in range(4):
            key_head(h, forget, value, margin, tri, run_row, fade, runs, kd, vv, state_out, decay_out)
    with jax.named_scope("met"):
        pl.semaphore_wait(barrier, 34)
    sems = (state_send, state_recv, decay_send, decay_recv)
    with jax.named_scope("state_send"):
        send_states(state_out, decay_out, state_in, decay_in, sems)
    with jax.named_scope("query"):
        copies[4].wait()
        query_pass(query, runs, run_col, qd, asked)
    with jax.named_scope("within"):
        within_pass(qd, kd, vv, run_row, run_col, local)
    back = (prior_send, prior_recv)
    with jax.named_scope("scan"):
        scan_states(state_in, decay_in, prior_out, prior_in, sems, back)
    with jax.named_scope("tables"):
        copies[5].wait()
        copies[6].wait()
        slot_tables(routes, weights, pack_l, comb_l)
    with jax.named_scope("factors"):
        copies[7].wait()
        copies[8].wait()
        gate_factors(gate_logits, head_scale, factor)
    with jax.named_scope("prior_wait"):
        wait_bytes(prior_in.at[pl.ds(0, 31)], prior_recv, False)
    gated = (gated_send, gated_recv)
    with jax.named_scope("gating"):
        gate_pass(asked, local, prior_in, factor, gated_out, gated_in, gated)
    for copy in copies[9:12]:
        copy.wait()
    with jax.named_scope("project"):
        project(gated_in, matrix, mixed, gated)
    stream = (resid[...].astype(F32) + mixed[...]).astype(BF16)
    resid[...] = stream
    values = stream.astype(F32)
    square = jnp.mean(values * values, axis=1, keepdims=True)
    normed = (values * lax.rsqrt(square + 1e-06) * scale[...]).astype(BF16)
    with jax.named_scope("experts"):
        expert_phase(resid, normed, pack_l, comb_l, gate, up, down, copies[12:], bufs, total, out)
    wait_bytes(state_out.at[pl.ds(0, 31)], state_send, True)
    wait_bytes(decay_in.at[pl.ds(0, 31)], decay_send, True)
    wait_bytes(prior_out.at[pl.ds(0, 31)], prior_send, True)
    wait_bytes(gated_out.at[pl.ds(0, 3)], gated_send, True)


def layer(
    resid, query, forget_logits, forget_margin, decay_spike, value_logits, output_gate_logits,
    head_norm_scale, output_matrix, norm_scale_vector, routes, routing_weight, gate, up, down,
):
    vmem = pl.BlockSpec(memory_space=pltpu.VMEM)
    hbm = pl.BlockSpec(memory_space=pl.ANY)
    dma = pltpu.SemaphoreType.DMA
    wide = pltpu.VMEM((512, 512), BF16)
    pieces = pltpu.VMEM((32, 16, 128), BF16)
    return pl.pallas_call(
        layer_kernel,
        out_shape=pltpu.VMEM((128, 2048), BF16),
        in_specs=[hbm] * 15,
        out_specs=vmem,
        scratch_shapes=[
            pltpu.VMEM((128, 2048), BF16),
            wide,
            wide,
            pltpu.VMEM((1, 512), F32),
            pltpu.VMEM((4, 512), F32),
            wide,
            wide,
            pltpu.VMEM((1, 512), F32),
            pltpu.VMEM((2048, 2048), BF16),
            pltpu.VMEM((1, 2048), F32),
            pltpu.VMEM((2, 128), I32),
            pltpu.VMEM((2, 128), F32),
            pltpu.VMEM((2048, 1024), BF16),
            pltpu.VMEM((2048, 1024), BF16),
            pltpu.VMEM((1024, 2048), BF16),
            dma((15,)),
            pltpu.VMEM((256, 256), BF16),
            pltpu.VMEM((512, 512), F32),
            pltpu.VMEM((512, 1024), BF16),
            pltpu.VMEM((512, 1024), BF16),
            wide,
            wide,
            pltpu.VMEM((8, 512), F32),
            pltpu.VMEM((512, 8), F32),
            pltpu.VMEM((512, 512), F32),
            pltpu.VMEM((512, 512), F32),
            pltpu.VMEM((128, 2048), F32),
            pltpu.VMEM((GROUPS, PER * 8, 256), BF16),
            pltpu.VMEM((GROUPS, PER * 8, 256), BF16),
            pltpu.VMEM((256, 1024), F32),
            pieces,
            pieces,
            pieces,
            pieces,
            pltpu.VMEM((4, 1, 128), F32),
            pltpu.VMEM((32, 1, 128), F32),
            pltpu.VMEM((4, 128, 512), BF16),
            pltpu.VMEM((4, 128, 512), BF16),
        ]
        + [dma] * 7
        + [dma((3,))]
        + slot_buffers(),
        compiler_params=pltpu.CompilerParams(
            collective_id=0, has_side_effects=True, vmem_limit_bytes=62 * 1024 * 1024
        ),
    )(
        resid, query, forget_logits, forget_margin.reshape(1, 512),
        decay_spike.T, value_logits, output_gate_logits,
        head_norm_scale.reshape(1, 512), output_matrix, norm_scale_vector.reshape(1, 2048),
        routes.T, routing_weight.T, gate, up, down,
    )


def solution(mesh):
    whole = ("sp", "tp")
    rows, heads, experts = P(whole, None), P("sp", "tp"), P(whole, None, None)
    return jax.shard_map(
        layer,
        mesh=mesh,
        in_specs=(
            rows, heads, heads, P("tp"), heads, heads, heads, P("tp"), P(), P(), rows, rows,
            experts, experts, experts,
        ),
        out_specs=rows,
        check_vma=False,
    )
```

```python
import jax
import jax.numpy as jnp
from jax import lax
from jax.experimental import pallas as pl
from jax.experimental.pallas import tpu as pltpu
from jax.sharding import PartitionSpec as P

MESH = pl.DeviceIdType.MESH
F32 = jnp.float32
BF16 = jnp.bfloat16
I32 = jnp.int32
GROUPS = 4
PER = 32


def coords():
    sp = lax.axis_index("sp")
    return sp // 8, (sp // 2) % 4, sp % 2, lax.axis_index("tp")


def wrap(value, size):
    return jnp.where(value >= size, value - size, value)


def entry_barrier():
    barrier = pltpu.get_barrier_semaphore()
    sp, x = lax.axis_index("sp"), lax.axis_index("tp")

    for low, top in ((16, 32), (1, 16)):

        @pl.loop(low, top)
        def _(p):
            pl.semaphore_signal(barrier, inc=1, device_id=(wrap(sp + p, 32), x), device_id_type=MESH)

    for k in range(1, 4):
        pl.semaphore_signal(barrier, inc=1, device_id=(sp, wrap(x + k, 4)), device_id_type=MESH)
    return barrier


def iota(shape, dim):
    return lax.broadcasted_iota(I32, shape, dim)


def slot_tables(routes, weights, pack_l, comb_l):
    z, y, c, x = coords()
    d = iota((128, 128), 0)
    dz, dy, dc = (d >> 3) & 3, (d >> 1) & 3, d & 1
    dx = ((d >> 5) + 8 - dz - dy) & 3
    expert = (((((z + dz) & 3) * 4 + ((y + dy) & 3)) * 2 + ((c + dc) & 1)) * 4) + ((x + dx) & 3)
    first = routes[0:1, :] == expert
    second = routes[1:2, :] == expert
    member = jnp.where(first, 1.0, jnp.where(second, 1.0, 0.0))
    earlier = jnp.where(iota((128, 128), 0) < iota((128, 128), 1), 1.0, 0.0).astype(BF16)
    rank = jnp.dot(member.astype(BF16), earlier, preferred_element_type=F32)
    code = (member * (rank + 1.0)).astype(BF16)
    share = jnp.where(first, weights[0:1, :], jnp.where(second, weights[1:2, :], 0.0))
    table = jnp.concatenate([code, share.astype(BF16)], axis=1)
    rows = PER * 8
    at = iota((rows, 128), 0)
    wanted = ((at & 3) + 1).astype(F32)
    upper = ((at >> 2) & 1) == 0
    for g in range(GROUPS):
        spread = jnp.where((at >> 3) + g * PER == iota((rows, 128), 1), 1.0, 0.0).astype(BF16)
        wide = jnp.dot(spread, table, preferred_element_type=F32)
        chosen = wide[:, :128] == wanted
        one = jnp.where(chosen, 1.0, 0.0)
        weighed = jnp.where(chosen, wide[:, 128:], 0.0)
        zero = jnp.zeros_like(one)
        pack_l[g] = jnp.concatenate(
            [jnp.where(upper, one, zero), jnp.where(upper, zero, one)], axis=1
        ).astype(BF16)
        comb_l[g] = jnp.concatenate(
            [jnp.where(upper, weighed, zero), jnp.where(upper, zero, weighed)], axis=1
        ).astype(BF16)


def blocks(ref, lo, count):
    return ref.at[pl.ds(lo, count)]


def wait_group(buf, sem, g):
    z, y, c, x = coords()
    other = (lax.axis_index("sp"), (x + 1) % 4)

    @pl.when(g == 0)
    def _():
        part = blocks(buf, 1, PER - 1)
        pltpu.make_async_remote_copy(part, part, sem, sem, other, MESH).wait_recv()

    @pl.when(g > 0)
    def _():
        part = blocks(buf, g * PER, PER)
        pltpu.make_async_remote_copy(part, part, sem, sem, other, MESH).wait_recv()


def send_group(src, dst, send_sem, recv_sem, g, sign):
    z, y, c, x = coords()
    turned = g if sign > 0 else 4 - g
    rows = [2 * wrap(y + (dy if sign > 0 else (4 - dy) % 4), 4) for dy in range(4)]
    cores = [c, 1 - c]

    def one(dz):
        plane = 8 * wrap(z + dz if sign > 0 else z + 4 - dz, 4)
        start = x + turned + (4 - dz if sign > 0 else dz)
        for dy in (2, 1, 3, 0):
            column = (start + (4 - dy if sign > 0 else dy)) % 4
            for dc in range(2):
                d = g * PER + dz * 8 + dy * 2 + dc
                copy = pltpu.make_async_remote_copy(
                    src.at[d], dst.at[d], send_sem, recv_sem,
                    (plane + rows[dy] + cores[dc], column), MESH,
                )
                if dy == 0 and dc == 0:
                    pl.when(d > 0)(copy.start)
                else:
                    copy.start()

    pl.loop(0, 4)(lambda k: one(wrap(k + 2, 4)))


def wait_sent(buf, sem):
    x = lax.axis_index("tp")
    part = blocks(buf, 1, GROUPS * PER - 1)
    pltpu.make_async_remote_copy(
        part, part, sem, sem, (lax.axis_index("sp"), (x + 1) % 4), MESH
    ).wait_send()


def expert_phase(stream, normed, pack_l, comb_l, gate, up, down, weight_copies, bufs, total, out):
    out_slots, in_slots, answers, replies, send_sem, recv_sem, send_back, recv_back = bufs
    halves = jnp.concatenate([normed[:, :1024], normed[:, 1024:]], axis=0)
    for g in range(GROUPS):
        with jax.named_scope("pack"):
            packed = jnp.dot(pack_l[g], halves, preferred_element_type=F32).astype(BF16)
            out_slots[pl.ds(g * PER, PER)] = packed.reshape(PER, 8, 1024)
        with jax.named_scope("dispatch"):
            send_group(out_slots, in_slots, send_sem, recv_sem.at[g], g, 1)
    in_slots[0] = out_slots[0]
    for copy in weight_copies:
        copy.wait()
    rows = PER * 8
    a, b = iota((rows, rows), 0), iota((rows, rows), 1)
    place = ((a & 127) >> 2) * 8 + (a >> 7) * 4 + (a & 3)
    unpack = jnp.where(place == b, 1.0, 0.0).astype(BF16)
    place_b = ((b & 127) >> 2) * 8 + (b >> 7) * 4 + (b & 3)
    repack = jnp.where(place_b == a, 1.0, 0.0).astype(BF16)

    @pl.loop(0, GROUPS)
    def _(g):
        with jax.named_scope("slots_wait"):
            wait_group(in_slots, recv_sem.at[g], g)
        came = in_slots[pl.ds(g * PER, PER)].reshape(rows, 1024)
        flat = jnp.dot(unpack, came, preferred_element_type=F32).astype(BF16)
        x = jnp.concatenate([flat[:128], flat[128:]], axis=1)
        hidden = []
        for n in range(0, 1024, 256):
            gated = jnp.dot(x, gate[:, n : n + 256], preferred_element_type=F32)
            lifted = jnp.dot(x, up[:, n : n + 256], preferred_element_type=F32)
            hidden.append((gated * logistic(gated) * lifted).astype(BF16))
        hidden = jnp.concatenate(hidden, axis=1)
        y0 = jnp.dot(hidden, down[:, :1024], preferred_element_type=F32).astype(BF16)
        y1 = jnp.dot(hidden, down[:, 1024:], preferred_element_type=F32).astype(BF16)
        both = jnp.concatenate([y0, y1], axis=0)
        back = jnp.dot(repack, both, preferred_element_type=F32).astype(BF16)
        answers[pl.ds(g * PER, PER)] = back.reshape(PER, 8, 1024)
        with jax.named_scope("answer_send"):
            send_group(answers, replies, send_back, recv_back.at[g], g, -1)

    replies[0] = answers[0]
    total[...] = jnp.zeros_like(total)

    def gathered(g):
        with jax.named_scope("replies_wait"):
            wait_group(replies, recv_back.at[g], g)
        return dot_tn(comb_l[g], replies[pl.ds(g * PER, PER)].reshape(rows, 1024))

    @pl.loop(0, GROUPS - 1)
    def _(g):
        total[...] += gathered(g)

    summed = total[...] + gathered(GROUPS - 1)
    for h in range(2):
        cols = slice(h * 1024, h * 1024 + 1024)
        out[:, cols] = (stream[:, cols].astype(F32) + summed[h * 128 : h * 128 + 128]).astype(BF16)
    wait_sent(out_slots, send_sem)
    wait_sent(answers, send_back)


def slot_buffers():
    slots = pltpu.VMEM((GROUPS * PER, 8, 1024), BF16)
    dma = pltpu.SemaphoreType.DMA
    return [slots] * 4 + [dma, dma((GROUPS,)), dma, dma((GROUPS,))]


def sp_peer(i):
    return (i, lax.axis_index("tp"))


def tp_peer(i):
    return (lax.axis_index("sp"), i)


def dot_nt(a, b):
    return lax.dot_general(a, b, (((1,), (1,)), ((), ())), preferred_element_type=F32)


def dot_tn(a, b):
    return lax.dot_general(a, b, (((0,), (0,)), ((), ())), preferred_element_type=F32)


def dot(a, b):
    return jnp.dot(a, b, preferred_element_type=F32)


def split(value):
    high = value.astype(BF16)
    return high, (value - high.astype(F32)).astype(BF16)


def logistic(value):
    return 0.5 * jnp.tanh(0.5 * value) + 0.5


def fill_triangle(tri):
    tri[...] = jnp.where(iota((256, 256), 0) >= iota((256, 256), 1), 1.0, 0.0).astype(BF16)


def spike_sums(spikes, tri, run_row, run_col):
    high, low = split(jnp.concatenate([spikes[...], jnp.zeros((4, 512), F32)], axis=0))
    parts = jnp.concatenate([high[:, :256], low[:, :256], high[:, 256:], low[:, 256:]], axis=0)
    sums = dot_nt(parts, tri[...])
    early = sums[:8] + sums[8:16]
    row = jnp.concatenate([early, sums[16:24] + sums[24:] + early[:, 255:256]], axis=1)
    run_row[...] = row
    run_col[...] = row.T


def key_head(h, forget, value, margin, tri, run_row, fade, runs, kd, vv, state_out, decay_out):
    cols = slice(h * 128, h * 128 + 128)
    keys = margin[:, cols] * logistic(-forget[:, cols].astype(F32))
    logs = jnp.concatenate(split(jnp.log1p(-keys)), axis=1)
    early, late = dot(tri[...], logs[:256]), dot(tri[...], logs[256:])
    early = early[:, :128] + early[:, 128:]
    run = jnp.concatenate([early, late[:, :128] + late[:, 128:] + early[255:]], axis=0)
    runs[:, cols] = run
    raised = keys * jnp.exp(-run)
    kd[:, cols] = raised.astype(BF16)
    logits = value[:, cols].astype(F32)
    values = (logits * logistic(logits)).astype(BF16)
    vv[:, cols] = values
    last = run[511:512]
    state = dot_tn(values, (raised * fade[:, h : h + 1]).astype(BF16)) * jnp.exp(last)
    state_out[pl.ds(h * 8, 8)] = state.astype(BF16).reshape(8, 16, 128)
    decay_out[h] = last + run_row[h : h + 1, 511:512]


def query_pass(query, runs, run_col, qd, asked):
    grow = jnp.exp(run_col[...])
    for h in range(4):
        cols = slice(h * 128, h * 128 + 128)
        faded = query[:, cols].astype(F32) * (jnp.exp(runs[:, cols]) * 128**-0.5)
        twice = slice(h * 256, h * 256 + 256)
        qd[:, twice] = jnp.concatenate(split(faded), axis=1)
        asked[:, twice] = jnp.concatenate(split(faded * grow[:, h : h + 1]), axis=1)


def within_pass(qd, kd, vv, run_row, run_col, local):
    causal = iota((128, 128), 0) >= iota((128, 128), 1)
    for h in range(4):
        cols = slice(h * 128, h * 128 + 128)
        for i in range(4):
            rows = slice(i * 128, i * 128 + 128)
            seen = (i + 1) * 128
            keys = kd[:seen, cols]
            scores = dot_nt(
                qd[rows, h * 256 : h * 256 + 256], jnp.concatenate([keys, keys], axis=1)
            )
            gap = run_col[rows, h : h + 1] - run_row[h : h + 1, :seen]
            edge = slice(i * 128, seen)
            inner = jnp.where(causal, scores[:, edge] * jnp.exp(jnp.where(causal, gap[:, edge], 0.0)), 0.0)
            parts = [inner.astype(BF16)]
            if i:
                parts.insert(0, (scores[:, : i * 128] * jnp.exp(gap[:, : i * 128])).astype(BF16))
            weights = jnp.concatenate(parts, axis=1)
            local[rows, cols] = dot(weights, vv[:seen, cols])


def send_states(state_out, decay_out, state_in, decay_in, sems):
    me = lax.axis_index("sp")
    send, recv, send_d, recv_d = sems
    for low, top in ((16, 32), (1, 16)):

        @pl.loop(low, top)
        def _(d):
            p = wrap(me + d, 32)
            pltpu.make_async_remote_copy(
                state_out.at[p], state_in.at[me], send, recv, sp_peer(p), MESH
            ).start()
            pltpu.make_async_remote_copy(
                decay_out.at[p // 8], decay_in.at[me], send_d, recv_d, sp_peer(p), MESH
            ).start()

    state_in[me] = state_out[me]
    decay_in[me] = decay_out[me // 8]


def wait_bytes(part, sem, sent):
    copy = pltpu.make_async_remote_copy(
        part, part, sem, sem, tp_peer((lax.axis_index("tp") + 1) % 4), MESH
    )
    if sent:
        copy.wait_send()
    else:
        copy.wait_recv()


def scan_states(state_in, decay_in, prior_out, prior_in, sems, back):
    send, recv, send_d, recv_d = sems
    wait_bytes(state_in.at[pl.ds(0, 31)], recv, False)
    wait_bytes(decay_in.at[pl.ds(0, 31)], recv_d, False)
    state = jnp.zeros((16, 128), F32)
    for i in range(32):
        prior_out[i] = state.astype(BF16)
        state = jnp.exp(decay_in[i]) * state + state_in[i].astype(F32)
    me = lax.axis_index("sp")

    for low, top in ((16, 32), (1, 16)):

        @pl.loop(low, top)
        def _(d):
            p = wrap(me + d, 32)
            pltpu.make_async_remote_copy(
                prior_out.at[p], prior_in.at[me], back[0], back[1], sp_peer(p), MESH
            ).start()

    prior_in[me] = prior_out[me]


def gate_factors(out_gate, head_scale, factor):
    logits = out_gate[...].astype(F32)
    factor[...] = head_scale[...] * (logits * logistic(logits))


def gate_pass(asked, local, prior_in, factor, gated_out, gated_in, sems):
    x = lax.axis_index("tp")
    for k, ahead in enumerate((2, 1, 3, 0)):
        j = wrap(x + ahead, 4)
        rows = pl.ds(pl.multiple_of(j * 128, 128), 128)
        for h in range(4):
            cols = slice(h * 128, h * 128 + 128)
            prior = prior_in[pl.ds(h * 8, 8)].reshape(128, 128)
            ask = asked[rows, h * 256 : h * 256 + 256]
            full = local[rows, cols] + dot_nt(ask, jnp.concatenate([prior, prior], axis=1))
            square = jnp.mean(full * full, axis=1, keepdims=True)
            gated_out[j, :, cols] = (full * lax.rsqrt(square + 1e-06) * factor[rows, cols]).astype(BF16)
        if ahead:
            pltpu.make_async_remote_copy(
                gated_out.at[j], gated_in.at[x], sems[0], sems[1].at[k], tp_peer(j), MESH
            ).start()
        else:
            gated_in[x] = gated_out[x]


def project(gated_in, matrix, resid, mixed, sems):
    x = lax.axis_index("tp")

    def product(i):
        return dot(gated_in[i], matrix[pl.ds(pl.multiple_of(i * 512, 512), 512)])

    mixed[...] = resid[...].astype(F32) + product(x)
    def arrived(k, back):
        i = wrap(x + back, 4)
        wait_bytes(gated_in.at[i], sems[1].at[k], False)
        return product(i)

    mixed[...] += arrived(0, 2)
    mixed[...] += arrived(1, 3)
    return (mixed[...] + arrived(2, 1)).astype(BF16)


def layer_kernel(
    resid_hbm, query_hbm, forget_hbm, margin_hbm, spikes_hbm, value_hbm, gate_logits_hbm, head_scale_hbm,
    matrix_hbm, scale_hbm, routes_hbm, weights_hbm, gate_hbm, up_hbm, down_hbm, out,
    resid, query, forget, margin, spikes, value, gate_logits, head_scale, matrix, scale, routes,
    weights, gate, up, down, in_sems,
    tri, runs, qd, asked, kd, vv, run_row, run_col, local, factor, mixed, pack_l, comb_l, total,
    state_out, state_in, prior_out, prior_in, decay_out, decay_in, gated_out, gated_in,
    state_send, state_recv, decay_send, decay_recv, prior_send, prior_recv, gated_send, gated_recv,
    *bufs,
):
    moves = [
        (spikes_hbm, spikes), (margin_hbm, margin), (forget_hbm, forget), (value_hbm, value),
        (query_hbm, query), (routes_hbm, routes), (weights_hbm, weights), (gate_logits_hbm, gate_logits),
        (head_scale_hbm, head_scale), (resid_hbm, resid), (scale_hbm, scale), (matrix_hbm, matrix),
        (gate_hbm.at[0], gate), (up_hbm.at[0], up), (down_hbm.at[0], down),
    ]
    copies = [pltpu.make_async_copy(src, dst, in_sems.at[i]) for i, (src, dst) in enumerate(moves)]
    for copy in copies[:5]:
        copy.start()
    with jax.named_scope("greet"):
        barrier = entry_barrier()
    for copy in copies[5:]:
        copy.start()
    with jax.named_scope("triangle"):
        fill_triangle(tri)
    copies[0].wait()
    with jax.named_scope("spikes"):
        spike_sums(spikes, tri, run_row, run_col)
        fade = jnp.exp(run_col[511:512, :] - run_col[...])
    with jax.named_scope("inputs"):
        for copy in copies[1:4]:
            copy.wait()
    with jax.named_scope("keys"):
        for h in range(4):
            key_head(h, forget, value, margin, tri, run_row, fade, runs, kd, vv, state_out, decay_out)
    with jax.named_scope("met"):
        pl.semaphore_wait(barrier, 34)
    sems = (state_send, state_recv, decay_send, decay_recv)
    with jax.named_scope("state_send"):
        send_states(state_out, decay_out, state_in, decay_in, sems)
    with jax.named_scope("query"):
        copies[4].wait()
        query_pass(query, runs, run_col, qd, asked)
    with jax.named_scope("within"):
        within_pass(qd, kd, vv, run_row, run_col, local)
    back = (prior_send, prior_recv)
    with jax.named_scope("scan"):
        scan_states(state_in, decay_in, prior_out, prior_in, sems, back)
    with jax.named_scope("tables"):
        copies[5].wait()
        copies[6].wait()
        slot_tables(routes, weights, pack_l, comb_l)
    with jax.named_scope("factors"):
        copies[7].wait()
        copies[8].wait()
        gate_factors(gate_logits, head_scale, factor)
    with jax.named_scope("prior_wait"):
        wait_bytes(prior_in.at[pl.ds(0, 31)], prior_recv, False)
    gated = (gated_send, gated_recv)
    with jax.named_scope("gating"):
        gate_pass(asked, local, prior_in, factor, gated_out, gated_in, gated)
    for copy in copies[9:12]:
        copy.wait()
    with jax.named_scope("project"):
        stream = project(gated_in, matrix, resid, mixed, gated)
    resid[...] = stream
    values = stream.astype(F32)
    square = jnp.mean(values * values, axis=1, keepdims=True)
    normed = (values * lax.rsqrt(square + 1e-06) * scale[...]).astype(BF16)
    with jax.named_scope("experts"):
        expert_phase(resid, normed, pack_l, comb_l, gate, up, down, copies[12:], bufs, total, out)
    wait_bytes(state_out.at[pl.ds(0, 31)], state_send, True)
    wait_bytes(decay_in.at[pl.ds(0, 31)], decay_send, True)
    wait_bytes(prior_out.at[pl.ds(0, 31)], prior_send, True)
    wait_bytes(gated_out.at[pl.ds(0, 3)], gated_send, True)


def layer(
    resid, query, forget_logits, forget_margin, decay_spike, value_logits, output_gate_logits,
    head_norm_scale, output_matrix, norm_scale_vector, routes, routing_weight, gate, up, down,
):
    vmem = pl.BlockSpec(memory_space=pltpu.VMEM)
    hbm = pl.BlockSpec(memory_space=pl.ANY)
    dma = pltpu.SemaphoreType.DMA
    wide = pltpu.VMEM((512, 512), BF16)
    pieces = pltpu.VMEM((32, 16, 128), BF16)
    return pl.pallas_call(
        layer_kernel,
        out_shape=pltpu.VMEM((128, 2048), BF16),
        in_specs=[hbm] * 15,
        out_specs=vmem,
        scratch_shapes=[
            pltpu.VMEM((128, 2048), BF16),
            wide,
            wide,
            pltpu.VMEM((1, 512), F32),
            pltpu.VMEM((4, 512), F32),
            wide,
            wide,
            pltpu.VMEM((1, 512), F32),
            pltpu.VMEM((2048, 2048), BF16),
            pltpu.VMEM((1, 2048), F32),
            pltpu.VMEM((2, 128), I32),
            pltpu.VMEM((2, 128), F32),
            pltpu.VMEM((2048, 1024), BF16),
            pltpu.VMEM((2048, 1024), BF16),
            pltpu.VMEM((1024, 2048), BF16),
            dma((15,)),
            pltpu.VMEM((256, 256), BF16),
            pltpu.VMEM((512, 512), F32),
            pltpu.VMEM((512, 1024), BF16),
            pltpu.VMEM((512, 1024), BF16),
            wide,
            wide,
            pltpu.VMEM((8, 512), F32),
            pltpu.VMEM((512, 8), F32),
            pltpu.VMEM((512, 512), F32),
            pltpu.VMEM((512, 512), F32),
            pltpu.VMEM((128, 2048), F32),
            pltpu.VMEM((GROUPS, PER * 8, 256), BF16),
            pltpu.VMEM((GROUPS, PER * 8, 256), BF16),
            pltpu.VMEM((256, 1024), F32),
            pieces,
            pieces,
            pieces,
            pieces,
            pltpu.VMEM((4, 1, 128), F32),
            pltpu.VMEM((32, 1, 128), F32),
            pltpu.VMEM((4, 128, 512), BF16),
            pltpu.VMEM((4, 128, 512), BF16),
        ]
        + [dma] * 7
        + [dma((3,))]
        + slot_buffers(),
        compiler_params=pltpu.CompilerParams(
            collective_id=0, has_side_effects=True, vmem_limit_bytes=62 * 1024 * 1024
        ),
    )(
        resid, query, forget_logits, forget_margin.reshape(1, 512),
        decay_spike.T, value_logits, output_gate_logits,
        head_norm_scale.reshape(1, 512), output_matrix, norm_scale_vector.reshape(1, 2048),
        routes.T, routing_weight.T, gate, up, down,
    )


def solution(mesh):
    whole = ("sp", "tp")
    rows, heads, experts = P(whole, None), P("sp", "tp"), P(whole, None, None)
    return jax.shard_map(
        layer,
        mesh=mesh,
        in_specs=(
            rows, heads, heads, P("tp"), heads, heads, heads, P("tp"), P(), P(), rows, rows,
            experts, experts, experts,
        ),
        out_specs=rows,
        check_vma=False,
    )
```

```python
import jax
import jax.numpy as jnp
from jax import lax
from jax.experimental import pallas as pl
from jax.experimental.pallas import tpu as pltpu
from jax.sharding import PartitionSpec as P

MESH = pl.DeviceIdType.MESH
F32 = jnp.float32
BF16 = jnp.bfloat16
I32 = jnp.int32
GROUPS = 4
PER = 32


def coords():
    sp = lax.axis_index("sp")
    return sp // 8, (sp // 2) % 4, sp % 2, lax.axis_index("tp")


def wrap(value, size):
    return jnp.where(value >= size, value - size, value)


def entry_barrier():
    barrier = pltpu.get_barrier_semaphore()
    sp, x = lax.axis_index("sp"), lax.axis_index("tp")

    for low, top in ((16, 32), (1, 16)):

        @pl.loop(low, top)
        def _(p):
            pl.semaphore_signal(barrier, inc=1, device_id=(wrap(sp + p, 32), x), device_id_type=MESH)

    for k in range(1, 4):
        pl.semaphore_signal(barrier, inc=1, device_id=(sp, wrap(x + k, 4)), device_id_type=MESH)
    return barrier


def iota(shape, dim):
    return lax.broadcasted_iota(I32, shape, dim)


def slot_tables(routes, weights, pack_l, comb_l):
    z, y, c, x = coords()
    d = iota((128, 128), 0)
    dz, dy, dc = (d >> 3) & 3, (d >> 1) & 3, d & 1
    dx = ((d >> 5) + 8 - dz - dy) & 3
    expert = (((((z + dz) & 3) * 4 + ((y + dy) & 3)) * 2 + ((c + dc) & 1)) * 4) + ((x + dx) & 3)
    first = routes[0:1, :] == expert
    second = routes[1:2, :] == expert
    member = jnp.where(first, 1.0, jnp.where(second, 1.0, 0.0))
    earlier = jnp.where(iota((128, 128), 0) < iota((128, 128), 1), 1.0, 0.0).astype(BF16)
    rank = jnp.dot(member.astype(BF16), earlier, preferred_element_type=F32)
    code = (member * (rank + 1.0)).astype(BF16)
    share = jnp.where(first, weights[0:1, :], jnp.where(second, weights[1:2, :], 0.0))
    table = jnp.concatenate([code, share.astype(BF16)], axis=1)
    rows = PER * 8
    at = iota((rows, 128), 0)
    wanted = ((at & 3) + 1).astype(F32)
    upper = ((at >> 2) & 1) == 0
    for g in range(GROUPS):
        spread = jnp.where((at >> 3) + g * PER == iota((rows, 128), 1), 1.0, 0.0).astype(BF16)
        wide = jnp.dot(spread, table, preferred_element_type=F32)
        chosen = wide[:, :128] == wanted
        one = jnp.where(chosen, 1.0, 0.0)
        weighed = jnp.where(chosen, wide[:, 128:], 0.0)
        zero = jnp.zeros_like(one)
        pack_l[g] = jnp.concatenate(
            [jnp.where(upper, one, zero), jnp.where(upper, zero, one)], axis=1
        ).astype(BF16)
        comb_l[g] = jnp.concatenate(
            [jnp.where(upper, weighed, zero), jnp.where(upper, zero, weighed)], axis=1
        ).astype(BF16)


def blocks(ref, lo, count):
    return ref.at[pl.ds(lo, count)]


def wait_group(buf, sem, g):
    z, y, c, x = coords()
    other = (lax.axis_index("sp"), (x + 1) % 4)

    @pl.when(g == 0)
    def _():
        part = blocks(buf, 1, PER - 1)
        pltpu.make_async_remote_copy(part, part, sem, sem, other, MESH).wait_recv()

    @pl.when(g > 0)
    def _():
        part = blocks(buf, g * PER, PER)
        pltpu.make_async_remote_copy(part, part, sem, sem, other, MESH).wait_recv()


def send_group(src, dst, send_sem, recv_sem, g, sign):
    z, y, c, x = coords()
    turned = g if sign > 0 else 4 - g
    rows = [2 * wrap(y + (dy if sign > 0 else (4 - dy) % 4), 4) for dy in range(4)]
    cores = [c, 1 - c]

    def one(dz):
        plane = 8 * wrap(z + dz if sign > 0 else z + 4 - dz, 4)
        start = x + turned + (4 - dz if sign > 0 else dz)
        for dy in (2, 1, 3, 0):
            column = (start + (4 - dy if sign > 0 else dy)) % 4
            for dc in range(2):
                d = g * PER + dz * 8 + dy * 2 + dc
                copy = pltpu.make_async_remote_copy(
                    src.at[d], dst.at[d], send_sem, recv_sem,
                    (plane + rows[dy] + cores[dc], column), MESH,
                )
                if dy == 0 and dc == 0:
                    pl.when(d > 0)(copy.start)
                else:
                    copy.start()

    pl.loop(0, 4)(lambda k: one(wrap(k + 2, 4)))


def wait_sent(buf, sem):
    x = lax.axis_index("tp")
    part = blocks(buf, 1, GROUPS * PER - 1)
    pltpu.make_async_remote_copy(
        part, part, sem, sem, (lax.axis_index("sp"), (x + 1) % 4), MESH
    ).wait_send()


def expert_phase(stream, normed, pack_l, comb_l, gate, up, down, weight_copies, bufs, total, out):
    out_slots, in_slots, answers, replies, send_sem, recv_sem, send_back, recv_back = bufs
    halves = jnp.concatenate([normed[:, :1024], normed[:, 1024:]], axis=0)
    for g in range(GROUPS):
        with jax.named_scope("pack"):
            packed = jnp.dot(pack_l[g], halves, preferred_element_type=F32).astype(BF16)
            out_slots[pl.ds(g * PER, PER)] = packed.reshape(PER, 8, 1024)
        with jax.named_scope("dispatch"):
            send_group(out_slots, in_slots, send_sem, recv_sem.at[g], g, 1)
    in_slots[0] = out_slots[0]
    for copy in weight_copies:
        copy.wait()
    rows = PER * 8
    a, b = iota((rows, rows), 0), iota((rows, rows), 1)
    place = ((a & 127) >> 2) * 8 + (a >> 7) * 4 + (a & 3)
    unpack = jnp.where(place == b, 1.0, 0.0).astype(BF16)
    place_b = ((b & 127) >> 2) * 8 + (b >> 7) * 4 + (b & 3)
    repack = jnp.where(place_b == a, 1.0, 0.0).astype(BF16)

    @pl.loop(0, GROUPS)
    def _(g):
        with jax.named_scope("slots_wait"):
            wait_group(in_slots, recv_sem.at[g], g)
        came = in_slots[pl.ds(g * PER, PER)].reshape(rows, 1024)
        flat = jnp.dot(unpack, came, preferred_element_type=F32).astype(BF16)
        x = jnp.concatenate([flat[:128], flat[128:]], axis=1)
        hidden = []
        for n in range(0, 1024, 256):
            gated = jnp.dot(x, gate[:, n : n + 256], preferred_element_type=F32)
            lifted = jnp.dot(x, up[:, n : n + 256], preferred_element_type=F32)
            hidden.append((gated * logistic(gated) * lifted).astype(BF16))
        hidden = jnp.concatenate(hidden, axis=1)
        y0 = jnp.dot(hidden, down[:, :1024], preferred_element_type=F32).astype(BF16)
        y1 = jnp.dot(hidden, down[:, 1024:], preferred_element_type=F32).astype(BF16)
        both = jnp.concatenate([y0, y1], axis=0)
        back = jnp.dot(repack, both, preferred_element_type=F32).astype(BF16)
        answers[pl.ds(g * PER, PER)] = back.reshape(PER, 8, 1024)
        with jax.named_scope("answer_send"):
            send_group(answers, replies, send_back, recv_back.at[g], g, -1)

    replies[0] = answers[0]
    total[...] = jnp.zeros_like(total)

    def gathered(g):
        with jax.named_scope("replies_wait"):
            wait_group(replies, recv_back.at[g], g)
        return dot_tn(comb_l[g], replies[pl.ds(g * PER, PER)].reshape(rows, 1024))

    @pl.loop(0, GROUPS - 1)
    def _(g):
        total[...] += gathered(g)

    summed = total[...] + gathered(GROUPS - 1)
    for h in range(2):
        cols = slice(h * 1024, h * 1024 + 1024)
        out[:, cols] = (stream[:, cols].astype(F32) + summed[h * 128 : h * 128 + 128]).astype(BF16)
    wait_sent(out_slots, send_sem)
    wait_sent(answers, send_back)


def slot_buffers():
    slots = pltpu.VMEM((GROUPS * PER, 8, 1024), BF16)
    dma = pltpu.SemaphoreType.DMA
    return [slots] * 4 + [dma, dma((GROUPS,)), dma, dma((GROUPS,))]


def sp_peer(i):
    return (i, lax.axis_index("tp"))


def tp_peer(i):
    return (lax.axis_index("sp"), i)


def dot_nt(a, b):
    return lax.dot_general(a, b, (((1,), (1,)), ((), ())), preferred_element_type=F32)


def dot_tn(a, b):
    return lax.dot_general(a, b, (((0,), (0,)), ((), ())), preferred_element_type=F32)


def dot(a, b):
    return jnp.dot(a, b, preferred_element_type=F32)


def split(value):
    high = value.astype(BF16)
    return high, (value - high.astype(F32)).astype(BF16)


def logistic(value):
    return 0.5 * jnp.tanh(0.5 * value) + 0.5


def fill_triangle(tri):
    tri[...] = jnp.where(iota((256, 256), 0) >= iota((256, 256), 1), 1.0, 0.0).astype(BF16)


def spike_sums(spikes, tri, run_row, run_col):
    high, low = split(jnp.concatenate([spikes[...], jnp.zeros((4, 512), F32)], axis=0))
    parts = jnp.concatenate([high[:, :256], low[:, :256], high[:, 256:], low[:, 256:]], axis=0)
    sums = dot_nt(parts, tri[...])
    early = sums[:8] + sums[8:16]
    row = jnp.concatenate([early, sums[16:24] + sums[24:] + early[:, 255:256]], axis=1)
    run_row[...] = row
    run_col[...] = row.T


def key_head(h, forget, value, margin, tri, run_row, fade, runs, kd, vv, state_out, decay_out):
    cols = slice(h * 128, h * 128 + 128)
    keys = margin[:, cols] * logistic(-forget[:, cols].astype(F32))
    logs = jnp.concatenate(split(jnp.log1p(-keys)), axis=1)
    early, late = dot(tri[...], logs[:256]), dot(tri[...], logs[256:])
    early = early[:, :128] + early[:, 128:]
    run = jnp.concatenate([early, late[:, :128] + late[:, 128:] + early[255:]], axis=0)
    runs[:, cols] = run
    raised = keys * jnp.exp(-run)
    kd[:, cols] = raised.astype(BF16)
    logits = value[:, cols].astype(F32)
    values = (logits * logistic(logits)).astype(BF16)
    vv[:, cols] = values
    last = run[511:512]
    state = dot_tn(values, (raised * fade[:, h : h + 1]).astype(BF16)) * jnp.exp(last)
    state_out[pl.ds(h * 8, 8)] = state.astype(BF16).reshape(8, 16, 128)
    decay_out[h] = last + run_row[h : h + 1, 511:512]


def query_pass(query, runs, run_col, qd, asked):
    grow = jnp.exp(run_col[...])
    for h in range(4):
        cols = slice(h * 128, h * 128 + 128)
        faded = query[:, cols].astype(F32) * (jnp.exp(runs[:, cols]) * 128**-0.5)
        twice = slice(h * 256, h * 256 + 256)
        qd[:, twice] = jnp.concatenate(split(faded), axis=1)
        asked[:, twice] = jnp.concatenate(split(faded * grow[:, h : h + 1]), axis=1)


def within_pass(qd, kd, vv, run_row, run_col, local):
    causal = iota((128, 128), 0) >= iota((128, 128), 1)
    for h in range(4):
        cols = slice(h * 128, h * 128 + 128)
        for i in range(4):
            rows = slice(i * 128, i * 128 + 128)
            seen = (i + 1) * 128
            keys = kd[:seen, cols]
            scores = dot_nt(
                qd[rows, h * 256 : h * 256 + 256], jnp.concatenate([keys, keys], axis=1)
            )
            gap = run_col[rows, h : h + 1] - run_row[h : h + 1, :seen]
            edge = slice(i * 128, seen)
            inner = jnp.where(causal, scores[:, edge] * jnp.exp(jnp.where(causal, gap[:, edge], 0.0)), 0.0)
            parts = [inner.astype(BF16)]
            if i:
                parts.insert(0, (scores[:, : i * 128] * jnp.exp(gap[:, : i * 128])).astype(BF16))
            weights = jnp.concatenate(parts, axis=1)
            local[rows, cols] = dot(weights, vv[:seen, cols])


def send_states(state_out, decay_out, state_in, decay_in, sems):
    me = lax.axis_index("sp")
    send, recv, send_d, recv_d = sems
    for low, top in ((16, 32), (1, 16)):

        @pl.loop(low, top)
        def _(d):
            p = (me + d * 11) % 32
            pltpu.make_async_remote_copy(
                state_out.at[p], state_in.at[me], send, recv, sp_peer(p), MESH
            ).start()
            pltpu.make_async_remote_copy(
                decay_out.at[p // 8], decay_in.at[me], send_d, recv_d, sp_peer(p), MESH
            ).start()

    state_in[me] = state_out[me]
    decay_in[me] = decay_out[me // 8]


def wait_bytes(part, sem, sent):
    copy = pltpu.make_async_remote_copy(
        part, part, sem, sem, tp_peer((lax.axis_index("tp") + 1) % 4), MESH
    )
    if sent:
        copy.wait_send()
    else:
        copy.wait_recv()


def scan_states(state_in, decay_in, prior_out, prior_in, sems, back):
    send, recv, send_d, recv_d = sems
    wait_bytes(state_in.at[pl.ds(0, 31)], recv, False)
    wait_bytes(decay_in.at[pl.ds(0, 31)], recv_d, False)
    state = jnp.zeros((16, 128), F32)
    for i in range(32):
        prior_out[i] = state.astype(BF16)
        state = jnp.exp(decay_in[i]) * state + state_in[i].astype(F32)
    me = lax.axis_index("sp")

    for low, top in ((16, 32), (1, 16)):

        @pl.loop(low, top)
        def _(d):
            p = (me + d * 11) % 32
            pltpu.make_async_remote_copy(
                prior_out.at[p], prior_in.at[me], back[0], back[1], sp_peer(p), MESH
            ).start()

    prior_in[me] = prior_out[me]


def gate_factors(out_gate, head_scale, factor):
    logits = out_gate[...].astype(F32)
    factor[...] = head_scale[...] * (logits * logistic(logits))


def gate_pass(asked, local, prior_in, factor, gated_out, gated_in, sems):
    x = lax.axis_index("tp")
    for k, ahead in enumerate((2, 1, 3, 0)):
        j = wrap(x + ahead, 4)
        rows = pl.ds(pl.multiple_of(j * 128, 128), 128)
        for h in range(4):
            cols = slice(h * 128, h * 128 + 128)
            prior = prior_in[pl.ds(h * 8, 8)].reshape(128, 128)
            ask = asked[rows, h * 256 : h * 256 + 256]
            full = local[rows, cols] + dot_nt(ask, jnp.concatenate([prior, prior], axis=1))
            square = jnp.mean(full * full, axis=1, keepdims=True)
            gated_out[j, :, cols] = (full * lax.rsqrt(square + 1e-06) * factor[rows, cols]).astype(BF16)
        if ahead:
            pltpu.make_async_remote_copy(
                gated_out.at[j], gated_in.at[x], sems[0], sems[1].at[k], tp_peer(j), MESH
            ).start()
        else:
            gated_in[x] = gated_out[x]


def project(gated_in, matrix, resid, mixed, sems):
    x = lax.axis_index("tp")

    def product(i):
        return dot(gated_in[i], matrix[pl.ds(pl.multiple_of(i * 512, 512), 512)])

    mixed[...] = resid[...].astype(F32) + product(x)
    def arrived(k, back):
        i = wrap(x + back, 4)
        wait_bytes(gated_in.at[i], sems[1].at[k], False)
        return product(i)

    mixed[...] += arrived(0, 2)
    mixed[...] += arrived(1, 3)
    return (mixed[...] + arrived(2, 1)).astype(BF16)


def layer_kernel(
    resid_hbm, query_hbm, forget_hbm, margin_hbm, spikes_hbm, value_hbm, gate_logits_hbm, head_scale_hbm,
    matrix_hbm, scale_hbm, routes_hbm, weights_hbm, gate_hbm, up_hbm, down_hbm, out,
    resid, query, forget, margin, spikes, value, gate_logits, head_scale, matrix, scale, routes,
    weights, gate, up, down, in_sems,
    tri, runs, qd, asked, kd, vv, run_row, run_col, local, factor, mixed, pack_l, comb_l, total,
    state_out, state_in, prior_out, prior_in, decay_out, decay_in, gated_out, gated_in,
    state_send, state_recv, decay_send, decay_recv, prior_send, prior_recv, gated_send, gated_recv,
    *bufs,
):
    moves = [
        (spikes_hbm, spikes), (margin_hbm, margin), (forget_hbm, forget), (value_hbm, value),
        (query_hbm, query), (routes_hbm, routes), (weights_hbm, weights), (gate_logits_hbm, gate_logits),
        (head_scale_hbm, head_scale), (resid_hbm, resid), (scale_hbm, scale), (matrix_hbm, matrix),
        (gate_hbm.at[0], gate), (up_hbm.at[0], up), (down_hbm.at[0], down),
    ]
    copies = [pltpu.make_async_copy(src, dst, in_sems.at[i]) for i, (src, dst) in enumerate(moves)]
    for copy in copies[:5]:
        copy.start()
    with jax.named_scope("greet"):
        barrier = entry_barrier()
    for copy in copies[5:]:
        copy.start()
    with jax.named_scope("triangle"):
        fill_triangle(tri)
    copies[0].wait()
    with jax.named_scope("spikes"):
        spike_sums(spikes, tri, run_row, run_col)
        fade = jnp.exp(run_col[511:512, :] - run_col[...])
    with jax.named_scope("inputs"):
        for copy in copies[1:4]:
            copy.wait()
    with jax.named_scope("keys"):
        for h in range(4):
            key_head(h, forget, value, margin, tri, run_row, fade, runs, kd, vv, state_out, decay_out)
    with jax.named_scope("met"):
        pl.semaphore_wait(barrier, 34)
    sems = (state_send, state_recv, decay_send, decay_recv)
    with jax.named_scope("state_send"):
        send_states(state_out, decay_out, state_in, decay_in, sems)
    with jax.named_scope("query"):
        copies[4].wait()
        query_pass(query, runs, run_col, qd, asked)
    with jax.named_scope("within"):
        within_pass(qd, kd, vv, run_row, run_col, local)
    back = (prior_send, prior_recv)
    with jax.named_scope("scan"):
        scan_states(state_in, decay_in, prior_out, prior_in, sems, back)
    with jax.named_scope("tables"):
        copies[5].wait()
        copies[6].wait()
        slot_tables(routes, weights, pack_l, comb_l)
    with jax.named_scope("factors"):
        copies[7].wait()
        copies[8].wait()
        gate_factors(gate_logits, head_scale, factor)
    with jax.named_scope("prior_wait"):
        wait_bytes(prior_in.at[pl.ds(0, 31)], prior_recv, False)
    gated = (gated_send, gated_recv)
    with jax.named_scope("gating"):
        gate_pass(asked, local, prior_in, factor, gated_out, gated_in, gated)
    for copy in copies[9:12]:
        copy.wait()
    with jax.named_scope("project"):
        stream = project(gated_in, matrix, resid, mixed, gated)
    resid[...] = stream
    values = stream.astype(F32)
    square = jnp.mean(values * values, axis=1, keepdims=True)
    normed = (values * lax.rsqrt(square + 1e-06) * scale[...]).astype(BF16)
    with jax.named_scope("experts"):
        expert_phase(resid, normed, pack_l, comb_l, gate, up, down, copies[12:], bufs, total, out)
    wait_bytes(state_out.at[pl.ds(0, 31)], state_send, True)
    wait_bytes(decay_in.at[pl.ds(0, 31)], decay_send, True)
    wait_bytes(prior_out.at[pl.ds(0, 31)], prior_send, True)
    wait_bytes(gated_out.at[pl.ds(0, 3)], gated_send, True)


def layer(
    resid, query, forget_logits, forget_margin, decay_spike, value_logits, output_gate_logits,
    head_norm_scale, output_matrix, norm_scale_vector, routes, routing_weight, gate, up, down,
):
    vmem = pl.BlockSpec(memory_space=pltpu.VMEM)
    hbm = pl.BlockSpec(memory_space=pl.ANY)
    dma = pltpu.SemaphoreType.DMA
    wide = pltpu.VMEM((512, 512), BF16)
    pieces = pltpu.VMEM((32, 16, 128), BF16)
    return pl.pallas_call(
        layer_kernel,
        out_shape=pltpu.VMEM((128, 2048), BF16),
        in_specs=[hbm] * 15,
        out_specs=vmem,
        scratch_shapes=[
            pltpu.VMEM((128, 2048), BF16),
            wide,
            wide,
            pltpu.VMEM((1, 512), F32),
            pltpu.VMEM((4, 512), F32),
            wide,
            wide,
            pltpu.VMEM((1, 512), F32),
            pltpu.VMEM((2048, 2048), BF16),
            pltpu.VMEM((1, 2048), F32),
            pltpu.VMEM((2, 128), I32),
            pltpu.VMEM((2, 128), F32),
            pltpu.VMEM((2048, 1024), BF16),
            pltpu.VMEM((2048, 1024), BF16),
            pltpu.VMEM((1024, 2048), BF16),
            dma((15,)),
            pltpu.VMEM((256, 256), BF16),
            pltpu.VMEM((512, 512), F32),
            pltpu.VMEM((512, 1024), BF16),
            pltpu.VMEM((512, 1024), BF16),
            wide,
            wide,
            pltpu.VMEM((8, 512), F32),
            pltpu.VMEM((512, 8), F32),
            pltpu.VMEM((512, 512), F32),
            pltpu.VMEM((512, 512), F32),
            pltpu.VMEM((128, 2048), F32),
            pltpu.VMEM((GROUPS, PER * 8, 256), BF16),
            pltpu.VMEM((GROUPS, PER * 8, 256), BF16),
            pltpu.VMEM((256, 1024), F32),
            pieces,
            pieces,
            pieces,
            pieces,
            pltpu.VMEM((4, 1, 128), F32),
            pltpu.VMEM((32, 1, 128), F32),
            pltpu.VMEM((4, 128, 512), BF16),
            pltpu.VMEM((4, 128, 512), BF16),
        ]
        + [dma] * 7
        + [dma((3,))]
        + slot_buffers(),
        compiler_params=pltpu.CompilerParams(
            collective_id=0, has_side_effects=True, vmem_limit_bytes=62 * 1024 * 1024
        ),
    )(
        resid, query, forget_logits, forget_margin.reshape(1, 512),
        decay_spike.T, value_logits, output_gate_logits,
        head_norm_scale.reshape(1, 512), output_matrix, norm_scale_vector.reshape(1, 2048),
        routes.T, routing_weight.T, gate, up, down,
    )


def solution(mesh):
    whole = ("sp", "tp")
    rows, heads, experts = P(whole, None), P("sp", "tp"), P(whole, None, None)
    return jax.shard_map(
        layer,
        mesh=mesh,
        in_specs=(
            rows, heads, heads, P("tp"), heads, heads, heads, P("tp"), P(), P(), rows, rows,
            experts, experts, experts,
        ),
        out_specs=rows,
        check_vma=False,
    )
```
